512 devices in a mesh: sp: 64 (over z, y), dp: 8 (over x, core).
Axes of the slice: x: 4, y: 8, z: 8, core: 2. Of those that a mesh axis runs over, the one named last changes fastest.
Arguments:
- glu_value: bfloat16 [8, 32768, 512], P('dp', 'sp'), may hold values from -6 to 6
- glu_gate: bfloat16 [8, 32768, 512], P('dp', 'sp'), may hold values from -8 to 8
- cotangent: bfloat16 [8, 32768, 2048], P('dp', 'sp'), may hold values from -8 to 8
- conv_weight: float32 [31, 512], replicated, may hold values from -1 to 1
- norm_gain: float32 [512], replicated, may hold values from 0.1 to 1.9
- norm_shift: float32 [512], replicated, may hold values from -3 to 3
- out_weight: bfloat16 [2048, 512], P('dp'), may hold values from -0.25 to 0.25
Outputs:
- grad_value: bfloat16 [8, 32768, 512], P('dp', 'sp')
- grad_gate: bfloat16 [8, 32768, 512], P('dp', 'sp')
- grad_out_weight: float32 [2048, 512], P('dp')
- grad_conv: float32 [31, 512], replicated
- grad_gain: float32 [512], replicated
- grad_shift: float32 [512], replicated
The draws below stay inside these ranges and needn't reach their ends.
All inputs are finite; a program needn't handle non-finite values.
Results may differ from the reference program's by a relative error of at most 0.003.
Values may be sent and summed in bfloat16 or wider, within the bound.
A program may use at most 64 MiB of HBM per device.

```python
import math
import jax
import jax.numpy as jnp
from jax import lax

D = 2048
C = 512
SPAN = 31
SEQS = 8
LENGTH = 32768
TOKENS = 262144


def strengthened(drawn, stream_key, source, target, shards_of, factor):
    owner, partner = [(jnp.arange(drawn.shape[dim]) // (drawn.shape[dim] // shards_of)).reshape([-1 if axis == dim else 1 for axis in range(drawn.ndim)]) for dim in (source, target)]
    chosen = jax.random.permutation(stream_key, shards_of)[partner]
    strong = (owner == chosen) | (owner == (partner + shards_of // 2) % shards_of)
    return jnp.where(strong, factor * drawn, drawn)


def steps_of(stream_key, extent, split, low, high):
    def one(position, shards_of):
        heights = jax.random.uniform(jax.random.fold_in(jax.random.fold_in(stream_key, 6), position), (shards_of,), jnp.float32, low / len(split), high / len(split))
        return jnp.repeat(jnp.exp(heights), extent[position] // shards_of).reshape((-1,) + (1,) * (len(extent) - position - 1))

    gain = one(*split[0])
    for cut in split[1:]:
        gain = gain * one(*cut)
    return gain


def scatter_about(stream_key, dims, width, limit, cuts=(), held_as=jnp.bfloat16):
    drawn = width * jax.random.normal(stream_key, dims, jnp.float32)
    if cuts:
        drawn = drawn * steps_of(stream_key, dims, cuts, -0.22, 0.18)
    return jnp.clip(drawn, -limit, limit).astype(held_as)


def bell_draw_with(own_key, dims, width, bound, split, heavy, kind=jnp.bfloat16):
    values = width * jax.random.normal(own_key, dims, jnp.float32)
    if split:
        values = values * steps_of(own_key, dims, split, -0.22, 0.18)
    return jnp.clip(strengthened(values, jax.random.fold_in(own_key, 3), *heavy), -bound, bound).astype(kind)


def setup_inputs(seed: int = 0) -> dict:
    keys = jax.random.split(jax.random.key(seed), 8)
    return {
        "glu_value": scatter_about(keys[0], (SEQS, LENGTH, C), 1.0, 6.0, ((0, 8), (1, 64))),
        "glu_gate": scatter_about(keys[1], (SEQS, LENGTH, C), 1.5, 8.0, ((0, 8), (1, 64))),
        "cotangent": bell_draw_with(keys[2], (SEQS, LENGTH, D), 1.0, 8.0, ((0, 8), (1, 64)), (1, 2, 64, 4.0)),
        "conv_weight": scatter_about(keys[3], (SPAN, C), SPAN ** -0.5, 1.0, (), jnp.float32),
        "norm_gain": jnp.clip(1.0 + 0.18 * jax.random.normal(keys[4], (C,), jnp.float32), 0.1, 1.9),
        "norm_shift": scatter_about(keys[5], (C,), 0.5, 3.0, (), jnp.float32),
        "out_weight": scatter_about(keys[6], (D, C), C ** -0.5, 0.25, ((0, 8),)),
    }


epsilon = 1e-06

def sequence_grads(value_rows, gate_rows, cotan_rows, conv_weight, norm_gain, norm_shift, out_weight):
    length = value_rows.shape[0]
    channels = value_rows.shape[1]
    tap_count = conv_weight.shape[0]
    value_full = value_rows.astype(jnp.float32)
    gate_full = gate_rows.astype(jnp.float32)
    sigmoid_gate = jax.nn.sigmoid(gate_full)
    gated = value_full * sigmoid_gate
    padded = jnp.concatenate([jnp.zeros((tap_count - 1, channels), jnp.float32), gated], axis=0)
    conv_rows = jnp.zeros((length, channels), jnp.float32)
    for offset in range(tap_count):
        conv_rows = conv_rows + conv_weight[offset] * padded[offset:offset + length]
    centred = conv_rows - lax.optimization_barrier(jnp.mean(conv_rows, axis=-1, keepdims=True))
    inv_std = lax.rsqrt(lax.optimization_barrier(jnp.mean(centred * centred, axis=-1, keepdims=True)) + epsilon)
    normed = centred * inv_std
    pre_act = normed * norm_gain + norm_shift
    sigmoid_pre = jax.nn.sigmoid(pre_act)
    act_rows = (pre_act * sigmoid_pre).astype(jnp.bfloat16)
    grad_act = jnp.dot(cotan_rows, out_weight, preferred_element_type=jnp.float32)
    grad_pre = grad_act * sigmoid_pre * (1.0 + pre_act * (1.0 - sigmoid_pre))
    grad_normed = grad_pre * norm_gain
    grad_conv_rows = inv_std * (grad_normed - lax.optimization_barrier(jnp.mean(grad_normed, axis=-1, keepdims=True)) - normed * lax.optimization_barrier(jnp.mean(grad_normed * normed, axis=-1, keepdims=True)))
    padded_grad = jnp.concatenate([grad_conv_rows, jnp.zeros((tap_count - 1, channels), jnp.float32)], axis=0)
    grad_gated = jnp.zeros((length, channels), jnp.float32)
    for offset in range(tap_count):
        start = tap_count - 1 - offset
        grad_gated = grad_gated + conv_weight[offset] * padded_grad[start:start + length]
    grad_taps = jnp.stack([lax.optimization_barrier(jnp.sum(grad_conv_rows * padded[offset:offset + length], axis=0)) for offset in range(tap_count)], axis=0)
    grad_value = (grad_gated * sigmoid_gate).astype(jnp.bfloat16)
    grad_gate = (grad_gated * value_full * sigmoid_gate * (1.0 - sigmoid_gate)).astype(jnp.bfloat16)
    grad_weight = jnp.dot(cotan_rows.T, act_rows, preferred_element_type=jnp.float32)
    return (grad_value, grad_gate, grad_weight, grad_taps, lax.optimization_barrier(jnp.sum(grad_pre * normed, axis=0)), lax.optimization_barrier(jnp.sum(grad_pre, axis=0)))

def reference(glu_value, glu_gate, cotangent, conv_weight, norm_gain, norm_shift, out_weight):

    def one_sequence(items):
        return sequence_grads(items[0], items[1], items[2], conv_weight, norm_gain, norm_shift, out_weight)
    results = lax.map(one_sequence, (glu_value, glu_gate, cotangent))
    scale = 1.0 / math.sqrt(TOKENS)
    grad_out_weight = lax.optimization_barrier(jnp.sum(results[2], axis=0)) * scale
    grad_conv = lax.optimization_barrier(jnp.sum(results[3], axis=0)) * scale
    grad_gain = lax.optimization_barrier(jnp.sum(results[4], axis=0)) * scale
    grad_shift = lax.optimization_barrier(jnp.sum(results[5], axis=0)) * scale
    return (results[0], results[1], grad_out_weight, grad_conv, grad_gain, grad_shift)
```

```python
import functools
import math

import jax
import jax.numpy as jnp
from jax import lax
from jax.experimental import pallas as pl
from jax.experimental.pallas import tpu as pltpu
from jax.sharding import PartitionSpec as P

MESH = pl.DeviceIdType.MESH
F32 = jnp.float32
BF16 = jnp.bfloat16

EPS = 1e-06
LANES = 128
HALO = 32
TILE = 64
SIDE = 8
CHIPS = 4
SMALL = 40
N_COPIES = 128


def sigmoid(x):
    return jax.nn.sigmoid(x)


def dot_t(a, b):
    return lax.dot_general(a, b, (((0,), (0,)), ((), ())), preferred_element_type=F32)


def kernel(
    scale, v_ref, g_ref, cot_ref, w_ref, gain_ref, shift_ref, ow_ref,
    gv_ref, gg_ref, gw_ref, sm_out,
    hv, hg, gated, normed, invs, dsil, ga, gcr, act, actp, cotp, wfull,
    stage, recvx, gsum, st_a, st_b, rs_a, rs_b, t_a, t_b, rt_a, rt_b, fin_a, fin_b,
    taps, acc_gs, sm_own, sm_par, sm_x, sm_2, sm_y, sm_z, sm_f,
    send_sems, recv_sems,
):
    rows, channels = v_ref.shape
    n_taps = w_ref.shape[0]
    blocks = channels // LANES
    features = ow_ref.shape[0]
    sp = lax.axis_index("sp")
    dp = lax.axis_index("dp")
    n_sp = SIDE * SIDE
    z, y = sp // SIDE, sp % SIDE
    x, core = dp // 2, dp % 2
    me_partner = {"sp": sp, "dp": 2 * x + (1 - core)}

    def at_x(k):
        return {"sp": sp, "dp": 2 * ((x + k) % CHIPS) + core}

    def at_y(k):
        return {"sp": z * SIDE + (y + k) % SIDE, "dp": dp}

    def at_z(k):
        return {"sp": ((z + k) % SIDE) * SIDE + y, "dp": dp}

    after = {"sp": (sp + 1) % n_sp, "dp": dp}
    before = {"sp": (sp + n_sp - 1) % n_sp, "dp": dp}

    counter = [0]
    started = []

    def send(src, dst, device):
        i = counter[0]
        counter[0] += 1
        copy = pltpu.make_async_remote_copy(
            src_ref=src, dst_ref=dst, send_sem=send_sems.at[i], recv_sem=recv_sems.at[i],
            device_id=device, device_id_type=MESH,
        )
        copy.start()
        started.append(copy)
        return copy

    barrier = pltpu.get_barrier_semaphore()
    peers = [me_partner, after, before]
    peers += [at_x(k) for k in range(1, CHIPS)]
    peers += [at_y(k) for k in range(1, SIDE)]
    peers += [at_z(k) for k in range(1, SIDE)]
    for peer in peers:
        pl.semaphore_signal(barrier, inc=1, device_id=peer, device_id_type=MESH)

    def lanes(cb):
        return slice(cb * LANES, (cb + 1) * LANES)

    def gate_tile(i, _):
        base = pl.multiple_of(i * TILE, TILE)
        for cb in range(blocks):
            v = v_ref[pl.ds(base, TILE), lanes(cb)].astype(F32)
            g = g_ref[pl.ds(base, TILE), lanes(cb)].astype(F32)
            gated[cb, pl.ds(base + HALO, TILE), :] = v * sigmoid(g)
        return 0

    lax.fori_loop(0, rows // TILE, gate_tile, 0)
    pl.semaphore_wait(barrier, len(peers))

    halo_v = send(v_ref.at[pl.ds(rows - HALO, HALO), :], hv, after)
    halo_g = send(g_ref.at[pl.ds(rows - HALO, HALO), :], hg, after)

    def shard(owner_x, owner_core):
        start = pl.multiple_of((2 * owner_x + owner_core) * features, features)
        return wfull.at[pl.ds(start, features), :]

    own_shard = shard(x, core)
    to_right = send(ow_ref, own_shard, at_x(1))
    to_left = send(ow_ref, own_shard, at_x(CHIPS - 1))
    to_other = send(ow_ref, own_shard, me_partner)

    def columns(owner_x, owner_core):
        return pl.ds(pl.multiple_of((2 * owner_x + owner_core) * features, features), features)

    cot_copies = [
        send(cot_ref.at[:, columns(k, 1 - core)], cotp.at[k], me_partner) for k in range(CHIPS)
    ]
    start = pl.multiple_of(dp * features, features)
    wfull[pl.ds(start, features), :] = ow_ref[...]

    def forward_tile(base):
        conv = []
        for cb in range(blocks):
            acc = jnp.zeros((TILE, LANES), F32)
            for j in range(n_taps):
                tap = w_ref[j : j + 1, lanes(cb)]
                acc = acc + tap * gated[cb, pl.ds(base + (j + HALO - n_taps + 1), TILE), :]
            conv.append(acc)
        total = functools.reduce(lambda a, b: a + b, conv)
        mean = jnp.sum(total, axis=-1, keepdims=True) * (1.0 / channels)
        centred = [c - mean for c in conv]
        squares = functools.reduce(lambda a, b: a + b, [c * c for c in centred])
        var = jnp.sum(squares, axis=-1, keepdims=True) * (1.0 / channels)
        inv = lax.rsqrt(var + EPS)
        invs[pl.ds(base, TILE), :] = jnp.broadcast_to(inv, (TILE, LANES))
        for cb in range(blocks):
            nrm = centred[cb] * inv
            pre = nrm * gain_ref[0:1, lanes(cb)] + shift_ref[0:1, lanes(cb)]
            sig = sigmoid(pre)
            normed[cb, pl.ds(base, TILE), :] = nrm
            act[pl.ds(base, TILE), lanes(cb)] = (pre * sig).astype(BF16)
            dsil[cb, pl.ds(base, TILE), :] = sig * (1.0 + pre * (1.0 - sig))

    def forward_step(i, _):
        forward_tile(pl.multiple_of(i * TILE, TILE))
        return 0

    lax.fori_loop(1, rows // TILE, forward_step, 0)
    halo_v.wait_recv()
    halo_g.wait_recv()
    inside = (sp > 0).astype(F32)
    for cb in range(blocks):
        v = hv[:, lanes(cb)].astype(F32)
        g = hg[:, lanes(cb)].astype(F32)
        gated[cb, pl.ds(0, HALO), :] = v * sigmoid(g) * inside
    lax.fori_loop(0, 1, forward_step, 0)
    act_copy = send(act, actp, me_partner)

    to_right.wait_recv()
    to_left.wait_recv()
    left_x, right_x = (x + CHIPS - 1) % CHIPS, (x + 1) % CHIPS
    pass_left = send(shard(left_x, core), shard(left_x, core), me_partner)
    pass_right = send(shard(right_x, core), shard(right_x, core), me_partner)
    source_x = (x + CHIPS - 1 + 2 * core) % CHIPS
    target_x = (x + 1 + 2 * core) % CHIPS
    pass_far = send(
        shard(source_x, core), shard(source_x, core), {"sp": sp, "dp": 2 * target_x + core}
    )

    for copy in cot_copies:
        copy.wait_recv()
    act_copy.wait_recv()
    x_copies = []
    for k in (2, 1, 3, 0):
        xt = (x + k) % CHIPS
        product = dot_t(cot_ref[:, columns(xt, core)], act[...]) + dot_t(cotp[xt], actp[...])
        if k:
            stage[k - 1] = product.astype(BF16)
            x_copies.append(send(stage.at[k - 1], recvx.at[k - 1], at_x(k)))
        else:
            gsum[...] = product

    pass_far.wait_recv()
    far_x = (x + 2) % CHIPS
    far_other = send(shard(far_x, core), shard(far_x, core), me_partner)
    to_other.wait_recv()
    pass_left.wait_recv()
    pass_right.wait_recv()
    far_other.wait_recv()

    half = rows // 2

    def matmul_step(i, _):
        base = pl.multiple_of(i * half, half)
        ga[pl.ds(base, half), :] = jnp.dot(
            cot_ref[pl.ds(base, half), :], wfull[...], preferred_element_type=F32
        )
        return 0

    lax.fori_loop(0, 2, matmul_step, 0)

    acc_gs[...] = jnp.zeros_like(acc_gs)
    taps[...] = jnp.zeros_like(taps)

    def fold(a):
        return a.reshape(TILE // 8, 8, LANES).sum(axis=0)

    def grad_step(i, _):
        base = pl.multiple_of(i * TILE, TILE)
        grads, norms = [], []
        for cb in range(blocks):
            gpre = ga[pl.ds(base, TILE), lanes(cb)] * dsil[cb, pl.ds(base, TILE), :]
            nrm = normed[cb, pl.ds(base, TILE), :]
            acc_gs[0, cb] = acc_gs[0, cb] + fold(gpre * nrm)
            acc_gs[1, cb] = acc_gs[1, cb] + fold(gpre)
            grads.append(gpre * gain_ref[0:1, lanes(cb)])
            norms.append(nrm)
        total = functools.reduce(lambda a, b: a + b, grads)
        mean = jnp.sum(total, axis=-1, keepdims=True) * (1.0 / channels)
        along = functools.reduce(lambda a, b: a + b, [a * b for a, b in zip(grads, norms)])
        mean_along = jnp.sum(along, axis=-1, keepdims=True) * (1.0 / channels)
        inv = invs[pl.ds(base, TILE), :]
        for cb in range(blocks):
            gcr[cb, pl.ds(base, TILE), :] = inv * (grads[cb] - mean - norms[cb] * mean_along)
        return 0

    lax.fori_loop(0, 1, grad_step, 0)
    halo_c = send(gcr.at[:, pl.ds(0, HALO), :], gcr.at[:, pl.ds(rows, HALO), :], before)
    lax.fori_loop(1, rows // TILE, grad_step, 0)

    def backward_step(i, _):
        base = pl.multiple_of(i * TILE, TILE)
        for cb in range(blocks):
            acc = jnp.zeros((TILE, LANES), F32)
            own = gated[cb, pl.ds(base + HALO, TILE), :]
            for j in range(n_taps):
                shifted = gcr[cb, pl.ds(base + j, TILE), :]
                acc = acc + w_ref[n_taps - 1 - j : n_taps - j, lanes(cb)] * shifted
                taps[cb, n_taps - 1 - j] = taps[cb, n_taps - 1 - j] + fold(own * shifted)
            v = v_ref[pl.ds(base, TILE), lanes(cb)].astype(F32)
            sig = sigmoid(g_ref[pl.ds(base, TILE), lanes(cb)].astype(F32))
            gs = acc * sig
            gv_ref[pl.ds(base, TILE), lanes(cb)] = gs.astype(BF16)
            gg_ref[pl.ds(base, TILE), lanes(cb)] = (gs * v * (1.0 - sig)).astype(BF16)
        return 0

    middle = rows // TILE // 2
    lax.fori_loop(0, middle, backward_step, 0)

    for copy in x_copies:
        copy.wait_recv()
    part = features // SIDE
    width = channels // 2
    for r in range(SIDE):
        piece = pl.ds(r * part, part)
        total = gsum[piece, :]
        for k in range(CHIPS - 1):
            total = total + recvx[k, piece, :].astype(F32)
        gsum[piece, :] = total
        st_a[r] = total[:, :width].astype(BF16)
        st_b[r] = total[:, width:].astype(BF16)
    order = (4, 3, 5, 2, 6, 1, 7)
    first_a, first_b = [], []
    for k in order:
        first_a.append(send(st_a.at[(y + k) % SIDE], rs_a.at[k - 1], at_y(k)))
        first_b.append(send(st_b.at[(z + k) % SIDE], rs_b.at[k - 1], at_z(k)))

    halo_c.wait_recv()
    beyond = (sp < n_sp - 1).astype(F32)
    for cb in range(blocks):
        gcr[cb, pl.ds(rows, HALO), :] = gcr[cb, pl.ds(rows, HALO), :] * beyond
    lax.fori_loop(middle, rows // TILE, backward_step, 0)

    per_block = SMALL // 8
    row_ids = lax.broadcasted_iota(jnp.int32, (8, LANES), 0)
    for t in range(24):
        cb, rb = t // per_block, t % per_block
        tile = jnp.zeros((8, LANES), F32)
        if cb < blocks:
            for r in range(8):
                j = rb * 8 + r
                if j < n_taps:
                    line = taps[cb, j]
                elif j < n_taps + 2:
                    line = acc_gs[j - n_taps, cb]
                else:
                    continue
                line = jnp.sum(line, axis=0, keepdims=True) * scale
                tile = jnp.where(row_ids == r, line, tile)
        sm_own[t // 3, t % 3] = tile
    small_other = send(sm_own, sm_par, me_partner)

    for copy in first_a + first_b:
        copy.wait_recv()

    def first_sum(own_index, rs, column, t_ref):
        total = gsum[pl.ds(pl.multiple_of(own_index * part, part), part), pl.ds(column, width)]
        for k in range(SIDE - 1):
            total = total + rs[k].astype(F32)
        total = total * scale
        for t in range(SIDE):
            r, c = t // 2, t % 2
            t_ref[t] = total[r * 8 : r * 8 + 8, c * LANES : (c + 1) * LANES]

    first_sum(y, rs_a, 0, t_a)
    first_sum(z, rs_b, width, t_b)
    second_a, second_b = [], []
    for k in order:
        second_a.append(send(t_a.at[(z + k) % SIDE], rt_a.at[k - 1], at_z(k)))
        second_b.append(send(t_b.at[(y + k) % SIDE], rt_b.at[k - 1], at_y(k)))

    small_other.wait_recv()
    sm_x[x] = sm_own[...] + sm_par[...]
    small_x = [send(sm_x.at[x], sm_x.at[x], at_x(k)) for k in (2, 1, 3)]

    for copy in second_a + second_b:
        copy.wait_recv()
    final_a, final_b = t_a[z], t_b[y]
    for k in range(SIDE - 1):
        final_a = final_a + rt_a[k]
        final_b = final_b + rt_b[k]
    fin_a[y, z] = final_a
    fin_b[z, y] = final_b
    spread_a, spread_b = [], []
    for k in order:
        spread_a.append(send(fin_a.at[y, z], fin_a.at[y, z], at_z(k)))
        spread_b.append(send(fin_b.at[z, y], fin_b.at[z, y], at_y(k)))

    for copy in small_x:
        copy.wait_recv()
    total = sm_x[0]
    for k in range(1, CHIPS):
        total = total + sm_x[k]
    sm_2[...] = total
    sm_y[y] = sm_2[y]
    small_y = [send(sm_2.at[(y + k) % SIDE], sm_y.at[y], at_y(k)) for k in order]

    for copy in spread_a + spread_b:
        copy.wait_recv()
    last_a, last_b = [], []
    for k in order:
        last_a.append(send(fin_a.at[y], fin_a.at[y], at_y(k)))
        last_b.append(send(fin_b.at[z], fin_b.at[z], at_z(k)))

    for copy in small_y:
        copy.wait_recv()
    total = sm_y[0]
    for k in range(1, SIDE):
        total = total + sm_y[k]
    sm_z[z] = total
    small_z = [send(sm_z.at[z], sm_z.at[z], at_z(k)) for k in order]
    for copy in small_z:
        copy.wait_recv()
    total = sm_z[0]
    for k in range(1, SIDE):
        total = total + sm_z[k]
    sm_f[y] = total
    small_f = [send(sm_f.at[y], sm_f.at[y], at_y(k)) for k in order]

    for copy in last_a + last_b:
        copy.wait_recv()
    for r in range(SIDE):
        for t in range(SIDE):
            line = slice(r * part + (t // 2) * 8, r * part + (t // 2) * 8 + 8)
            c = (t % 2) * LANES
            gw_ref[line, c : c + LANES] = fin_a[r, t]
            gw_ref[line, width + c : width + c + LANES] = fin_b[r, t]

    for copy in small_f:
        copy.wait_recv()
    for t in range(blocks * per_block):
        cb, rb = t // per_block, t % per_block
        sm_out[rb * 8 : rb * 8 + 8, lanes(cb)] = sm_f[t // 3, t % 3]
    for copy in started:
        copy.wait_send()


def per_device(count, glu_value, glu_gate, cotangent, conv_weight, norm_gain, norm_shift, out_weight):
    value, gate, cot = glu_value[0], glu_gate[0], cotangent[0]
    rows, channels = value.shape
    n_taps = conv_weight.shape[0]
    features = out_weight.shape[0]
    blocks = channels // LANES
    part, width = features // SIDE, channels // 2
    scale = 1.0 / math.sqrt(rows * count)
    vmem = pl.BlockSpec(memory_space=pltpu.VMEM)
    shape = jax.ShapeDtypeStruct
    tile = (8, LANES)
    small = (SIDE, 3, *tile)
    outs = pl.pallas_call(
        functools.partial(kernel, scale),
        out_shape=[
            shape((rows, channels), BF16),
            shape((rows, channels), BF16),
            shape((features, channels), F32),
            shape((SMALL, channels), F32),
        ],
        in_specs=[vmem] * 7,
        out_specs=[vmem] * 4,
        scratch_shapes=[
            pltpu.VMEM((HALO, channels), BF16),
            pltpu.VMEM((HALO, channels), BF16),
            pltpu.VMEM((blocks, rows + HALO, LANES), F32),
            pltpu.VMEM((blocks, rows, LANES), F32),
            pltpu.VMEM((rows, LANES), F32),
            pltpu.VMEM((blocks, rows, LANES), F32),
            pltpu.VMEM((rows, channels), F32),
            pltpu.VMEM((blocks, rows + HALO, LANES), F32),
            pltpu.VMEM((rows, channels), BF16),
            pltpu.VMEM((rows, channels), BF16),
            pltpu.VMEM((CHIPS, rows, features), BF16),
            pltpu.VMEM((2 * CHIPS * features, channels), BF16),
            pltpu.VMEM((CHIPS - 1, features, channels), BF16),
            pltpu.VMEM((CHIPS - 1, features, channels), BF16),
            pltpu.VMEM((features, channels), F32),
            pltpu.VMEM((SIDE, part, width), BF16),
            pltpu.VMEM((SIDE, part, width), BF16),
            pltpu.VMEM((SIDE - 1, part, width), BF16),
            pltpu.VMEM((SIDE - 1, part, width), BF16),
            pltpu.VMEM((SIDE, *tile), F32),
            pltpu.VMEM((SIDE, *tile), F32),
            pltpu.VMEM((SIDE - 1, *tile), F32),
            pltpu.VMEM((SIDE - 1, *tile), F32),
            pltpu.VMEM((SIDE, SIDE, *tile), F32),
            pltpu.VMEM((SIDE, SIDE, *tile), F32),
            pltpu.VMEM((blocks, n_taps, *tile), F32),
            pltpu.VMEM((2, blocks, *tile), F32),
            pltpu.VMEM(small, F32),
            pltpu.VMEM(small, F32),
            pltpu.VMEM((CHIPS, *small), F32),
            pltpu.VMEM(small, F32),
            pltpu.VMEM(small, F32),
            pltpu.VMEM(small, F32),
            pltpu.VMEM(small, F32),
            pltpu.SemaphoreType.DMA((N_COPIES,)),
            pltpu.SemaphoreType.DMA((N_COPIES,)),
        ],
        compiler_params=pltpu.CompilerParams(
            collective_id=0, has_side_effects=True, vmem_limit_bytes=60 * 2**20
        ),
        name="backward",
    )(value, gate, cot, conv_weight, norm_gain[None], norm_shift[None], out_weight)
    grad_value, grad_gate, grad_weight, lines = outs
    return (
        grad_value[None],
        grad_gate[None],
        grad_weight,
        lines[:n_taps],
        lines[n_taps],
        lines[n_taps + 1],
    )


def solution(mesh):
    return jax.shard_map(
        functools.partial(per_device, mesh.size),
        mesh=mesh,
        in_specs=(
            P("dp", "sp", None), P("dp", "sp", None), P("dp", "sp", None),
            P(), P(), P(), P("dp", None),
        ),
        out_specs=(P("dp", "sp", None), P("dp", "sp", None), P("dp", None), P(), P(), P()),
        check_vma=False,
    )
```

```python
import functools
import math

import jax
import jax.numpy as jnp
from jax import lax
from jax.experimental import pallas as pl
from jax.experimental.pallas import tpu as pltpu
from jax.sharding import PartitionSpec as P

MESH = pl.DeviceIdType.MESH
F32 = jnp.float32
BF16 = jnp.bfloat16

EPS = 1e-06
LANES = 128
HALO = 32
TILE = 64
SIDE = 8
CHIPS = 4
COPIES = 160
SMALL = 40
OWN_TILES = 3
ORDER = (4, 3, 5, 2, 6, 1, 7)
NEAR_FIRST = (1, 7, 2, 6, 3, 5, 4)


class Phases:
    def __init__(self):
        self.open = None

    def __call__(self, name):
        if self.open is not None:
            self.open.__exit__(None, None, None)
        self.open = None
        if name is not None:
            self.open = jax.named_scope(name)
            self.open.__enter__()


def sigmoid(x):
    return jax.nn.sigmoid(x)


def dot_t(a, b):
    return lax.dot_general(a, b, (((0,), (0,)), ((), ())), preferred_element_type=F32)


def added(terms):
    return functools.reduce(lambda a, b: a + b, terms)


def kernel(
    scale, v_hbm, g_hbm, cot_hbm, w_hbm, gain_hbm, shift_hbm, ow_hbm,
    gv_out, gg_out, gw_out, sm_out,
    v_ref, g_ref, cot_ref, w_ref, gain_ref, shift_ref, ow_ref, gv_ref, gg_ref, gw_ref, lines,
    hv, hg, gated, normed, invs, dsil, ga, gcr, act, actp, cotp, wfull,
    far_st, opp_st, near_st, far_in, opp_in, near_in, near_own, gsum, spread_st, spread_in,
    t_a, t_b, rt_a, rt_b, fin_a, fin_b,
    taps, acc_gs, sm_all, sm_in, sm_ya, sm_zb, sm_za, sm_yb, sm_fin,
    send_sems, recv_sems, local_sems,
):
    phase = Phases()
    phase("start")
    rows, channels = v_ref.shape
    n_taps = w_ref.shape[0]
    blocks = channels // LANES
    features = ow_ref.shape[0]
    sp = lax.axis_index("sp")
    dp = lax.axis_index("dp")
    n_sp, n_dp = SIDE * SIDE, 2 * CHIPS
    z, y = sp // SIDE, sp % SIDE
    x, core = dp // 2, dp % 2
    step_x = 1 - 2 * core
    ahead_x = (x + CHIPS + step_x) % CHIPS
    behind_x = (x + CHIPS - step_x) % CHIPS
    far_x = (x + 2) % CHIPS

    other = {"sp": sp, "dp": 2 * x + (1 - core)}
    after = {"sp": (sp + 1) % n_sp, "dp": dp}
    before = {"sp": (sp + n_sp - 1) % n_sp, "dp": dp}
    at_y = {k: {"sp": z * SIDE + (y + k) % SIDE, "dp": dp} for k in range(1, SIDE)}
    at_z = {k: {"sp": ((z + k) % SIDE) * SIDE + y, "dp": dp} for k in range(1, SIDE)}
    at_dp = {k: {"sp": sp, "dp": (dp + k) % n_dp} for k in range(1, n_dp)}

    def chip(where):
        return {"sp": sp, "dp": 2 * where + core}

    barrier = pltpu.get_barrier_semaphore()
    peers = [after, before, *at_dp.values(), *at_y.values(), *at_z.values()]
    for peer in peers:
        pl.semaphore_signal(barrier, inc=1, device_id=peer, device_id_type=MESH)

    counter = [0, 0]
    started = []

    def remote(src, dst, device, i):
        return pltpu.make_async_remote_copy(
            src_ref=src, dst_ref=dst, send_sem=send_sems.at[i], recv_sem=recv_sems.at[i],
            device_id=device, device_id_type=MESH,
        )

    def send(src, dst, device):
        copy = remote(src, dst, device, counter[0])
        counter[0] += 1
        copy.start()
        started.append(copy)
        return copy

    def local(src, dst):
        copy = pltpu.make_async_copy(src, dst, local_sems.at[counter[1]])
        counter[1] += 1
        copy.start()
        return copy

    loads = [
        local(v_hbm, v_ref), local(g_hbm, g_ref), local(ow_hbm, ow_ref), local(cot_hbm, cot_ref),
        local(w_hbm, w_ref), local(gain_hbm, gain_ref), local(shift_hbm, shift_ref),
    ]

    def lanes(cb):
        return slice(cb * LANES, (cb + 1) * LANES)

    def gate_tile(i, _):
        base = pl.multiple_of(i * TILE, TILE)
        for cb in range(blocks):
            v = v_ref[pl.ds(base, TILE), lanes(cb)].astype(F32)
            g = g_ref[pl.ds(base, TILE), lanes(cb)].astype(F32)
            gated[cb, pl.ds(base + HALO, TILE), :] = v * sigmoid(g)
        return 0

    phase("loads")
    loads[0].wait()
    loads[1].wait()
    phase("gate")
    lax.fori_loop(0, rows // TILE, gate_tile, 0)
    phase("loads2")
    for copy in loads[2:]:
        copy.wait()
    phase("barrier")
    pl.semaphore_wait(barrier, len(peers))
    phase("issue")

    halo_v = send(v_ref.at[pl.ds(rows - HALO, HALO), :], hv, after)
    halo_g = send(g_ref.at[pl.ds(rows - HALO, HALO), :], hg, after)

    def columns(owner_x, owner_core):
        return pl.ds(pl.multiple_of((2 * owner_x + owner_core) * features, features), features)

    def shard(owner_x, owner_core):
        return wfull.at[columns(owner_x, owner_core), :]

    to_ahead = send(ow_ref, shard(x, core), chip(ahead_x))
    to_behind = send(ow_ref, shard(x, core), chip(behind_x))
    to_other = send(ow_ref, shard(x, core), other)
    cot_copies = [
        send(cot_ref.at[:, columns(k, 1 - core)], cotp.at[k], other) for k in range(CHIPS)
    ]
    wfull[columns(x, core), :] = ow_ref[...]

    def forward_step(i, _):
        base = pl.multiple_of(i * TILE, TILE)
        conv = []
        for cb in range(blocks):
            acc = jnp.zeros((TILE, LANES), F32)
            for j in range(n_taps):
                tap = w_ref[j : j + 1, lanes(cb)]
                acc = acc + tap * gated[cb, pl.ds(base + (j + HALO - n_taps + 1), TILE), :]
            conv.append(acc)
        mean = jnp.sum(added(conv), axis=-1, keepdims=True) * (1.0 / channels)
        centred = [c - mean for c in conv]
        var = jnp.sum(added([c * c for c in centred]), axis=-1, keepdims=True) * (1.0 / channels)
        inv = lax.rsqrt(var + EPS)
        invs[pl.ds(base, TILE), :] = jnp.broadcast_to(inv, (TILE, LANES))
        for cb in range(blocks):
            nrm = centred[cb] * inv
            pre = nrm * gain_ref[0:1, lanes(cb)] + shift_ref[0:1, lanes(cb)]
            sig = sigmoid(pre)
            normed[cb, pl.ds(base, TILE), :] = nrm
            act[pl.ds(base, TILE), lanes(cb)] = (pre * sig).astype(BF16)
            dsil[cb, pl.ds(base, TILE), :] = sig * (1.0 + pre * (1.0 - sig))
        return 0

    phase("forward")
    lax.fori_loop(1, rows // TILE, forward_step, 0)
    phase("halo_wait")
    halo_v.wait_recv()
    halo_g.wait_recv()
    phase("forward0")
    inside = (sp > 0).astype(F32)
    for cb in range(blocks):
        v = hv[:, lanes(cb)].astype(F32)
        g = hg[:, lanes(cb)].astype(F32)
        gated[cb, pl.ds(0, HALO), :] = v * sigmoid(g) * inside
    lax.fori_loop(0, 1, forward_step, 0)
    act_copy = send(act, actp, other)

    phase("act_wait")
    for copy in cot_copies:
        copy.wait_recv()
    act_copy.wait_recv()
    phase("product")
    pieces = (0, 2, 1, 3)

    def product(owner_x):
        cols = columns(owner_x, core)
        return dot_t(cot_ref[:, cols], act[...]) + dot_t(cotp[owner_x], actp[...])

    value = product(far_x).astype(BF16)
    for p in range(blocks):
        far_st[p] = value[:, lanes(p)]
    far_copies = {p: send(far_st.at[p], far_in.at[p], chip(ahead_x)) for p in pieces}
    value = product(behind_x).astype(BF16)
    for p in range(blocks):
        opp_st[p] = value[:, lanes(p)]
    opp_copies = {p: send(opp_st.at[p], opp_in.at[p], chip(behind_x)) for p in pieces}
    near_own[...] = product(ahead_x)
    gsum[...] = product(x)

    phase("w_wait1")
    to_ahead.wait_recv()
    to_behind.wait_recv()
    pass_far = send(shard(behind_x, core), shard(behind_x, core), chip(ahead_x))
    pass_1 = send(shard(behind_x, core), shard(behind_x, core), other)
    pass_2 = send(shard(ahead_x, core), shard(ahead_x, core), other)

    near_copies = {}

    def relay(p):
        far_copies[p].wait_recv()
        near_st[p] = (near_own[:, lanes(p)] + far_in[p].astype(F32)).astype(BF16)
        near_copies[p] = send(near_st.at[p], near_in.at[p], chip(ahead_x))

    phase("relay1")
    relay(0)
    relay(2)
    phase("w_wait2")
    pass_far.wait_recv()
    far_other = send(shard(far_x, core), shard(far_x, core), other)
    phase("relay2")
    relay(1)
    relay(3)
    phase("w_wait3")
    to_other.wait_recv()
    pass_1.wait_recv()
    pass_2.wait_recv()
    far_other.wait_recv()

    phase("matmul")
    half = rows // 2

    def matmul_step(i, _):
        base = pl.multiple_of(i * half, half)
        ga[pl.ds(base, half), :] = jnp.dot(
            cot_ref[pl.ds(base, half), :], wfull[...], preferred_element_type=F32
        )
        return 0

    lax.fori_loop(0, 2, matmul_step, 0)
    phase("grad")
    acc_gs[...] = jnp.zeros_like(acc_gs)
    taps[...] = jnp.zeros_like(taps)

    def fold(a):
        return a.reshape(TILE // 8, 8, LANES).sum(axis=0)

    def grad_step(i, _):
        base = pl.multiple_of(i * TILE, TILE)
        grads, norms = [], []
        for cb in range(blocks):
            gpre = ga[pl.ds(base, TILE), lanes(cb)] * dsil[cb, pl.ds(base, TILE), :]
            nrm = normed[cb, pl.ds(base, TILE), :]
            acc_gs[0, cb] = acc_gs[0, cb] + fold(gpre * nrm)
            acc_gs[1, cb] = acc_gs[1, cb] + fold(gpre)
            grads.append(gpre * gain_ref[0:1, lanes(cb)])
            norms.append(nrm)
        mean = jnp.sum(added(grads), axis=-1, keepdims=True) * (1.0 / channels)
        along = added([a * b for a, b in zip(grads, norms)])
        mean_along = jnp.sum(along, axis=-1, keepdims=True) * (1.0 / channels)
        inv = invs[pl.ds(base, TILE), :]
        for cb in range(blocks):
            gcr[cb, pl.ds(base, TILE), :] = inv * (grads[cb] - mean - norms[cb] * mean_along)
        return 0

    lax.fori_loop(0, 1, grad_step, 0)
    halo_c = send(gcr.at[:, pl.ds(0, HALO), :], gcr.at[:, pl.ds(rows, HALO), :], before)
    lax.fori_loop(1, rows // TILE, grad_step, 0)

    part = features // SIDE

    spread_copies = {}

    def chip_sum(p):
        near_copies[p].wait_recv()
        opp_copies[p].wait_recv()
        total = gsum[:, lanes(p)] + near_in[p].astype(F32) + opp_in[p].astype(F32)
        gsum[:, lanes(p)] = total
        spread_st[p] = total.astype(BF16)
        mine, at = (y, at_y) if p < 2 else (z, at_z)
        for k in ORDER:
            chunk = pl.ds(pl.multiple_of(((mine + k) % SIDE) * part, part), part)
            spread_copies[p, k] = send(spread_st.at[p, chunk, :], spread_in.at[p, k - 1], at[k])

    phase("chip_sum1")
    chip_sum(0)
    chip_sum(2)

    def taps_step(i, _):
        base = pl.multiple_of(i * TILE, TILE)
        for cb in range(blocks):
            own = gated[cb, pl.ds(base + HALO, TILE), :]
            for j in range(n_taps):
                shifted = gcr[cb, pl.ds(base + (n_taps - 1 - j), TILE), :]
                taps[cb, j] = taps[cb, j] + fold(own * shifted)
        return 0

    n_tiles = rows // TILE
    phase("taps1")
    lax.fori_loop(0, n_tiles // 2, taps_step, 0)
    phase("chip_sum2")
    chip_sum(1)
    chip_sum(3)
    phase("halo_c")
    halo_c.wait_recv()
    beyond = (sp < n_sp - 1).astype(F32)
    for cb in range(blocks):
        gcr[cb, pl.ds(rows, HALO), :] = gcr[cb, pl.ds(rows, HALO), :] * beyond
    phase("taps2")
    lax.fori_loop(n_tiles // 2, n_tiles, taps_step, 0)

    phase("small_fold")
    per_block = SMALL // 8
    row_ids = lax.broadcasted_iota(jnp.int32, (8, LANES), 0)
    for t in range(n_dp * OWN_TILES):
        cb, rb = t // per_block, t % per_block
        tile = jnp.zeros((8, LANES), F32)
        if cb < blocks:
            for r in range(8):
                j = rb * 8 + r
                if j < n_taps:
                    line = taps[cb, j]
                elif j < n_taps + 2:
                    line = acc_gs[j - n_taps, cb]
                else:
                    continue
                line = jnp.sum(line, axis=0, keepdims=True) * scale
                tile = jnp.where(row_ids == r, line, tile)
        sm_all[t // OWN_TILES, t % OWN_TILES] = tile
    small_rs = [send(sm_all.at[(dp + k) % n_dp], sm_in.at[k - 1], at_dp[k]) for k in range(1, n_dp)]

    def backward_step(i, _):
        base = pl.multiple_of(i * TILE, TILE)
        for cb in range(blocks):
            acc = jnp.zeros((TILE, LANES), F32)
            for j in range(n_taps):
                tap = w_ref[j : j + 1, lanes(cb)]
                acc = acc + tap * gcr[cb, pl.ds(base + (n_taps - 1 - j), TILE), :]
            v = v_ref[pl.ds(base, TILE), lanes(cb)].astype(F32)
            sig = sigmoid(g_ref[pl.ds(base, TILE), lanes(cb)].astype(F32))
            gs = acc * sig
            gv_ref[pl.ds(base, TILE), lanes(cb)] = gs.astype(BF16)
            gg_ref[pl.ds(base, TILE), lanes(cb)] = (gs * v * (1.0 - sig)).astype(BF16)
        return 0

    phase("rs1_wait")
    for copy in spread_copies.values():
        copy.wait_recv()
    phase("rs1_sum")

    def first_sum(own_index, first_piece, t_ref):
        chunk = pl.ds(pl.multiple_of(own_index * part, part), part)
        for c in range(2):
            p = first_piece + c
            total = gsum[chunk, lanes(p)]
            for k in range(SIDE - 1):
                total = total + spread_in[p, k].astype(F32)
            total = total * scale
            for r in range(part // 8):
                t_ref[2 * r + c] = total[r * 8 : r * 8 + 8, :]

    first_sum(y, 0, t_a)
    first_sum(z, 2, t_b)
    second_a, second_b = [], []
    for k in ORDER:
        second_a.append(send(t_a.at[(z + k) % SIDE], rt_a.at[k - 1], at_z[k]))
        second_b.append(send(t_b.at[(y + k) % SIDE], rt_b.at[k - 1], at_y[k]))

    phase("backward1")
    lax.fori_loop(0, n_tiles // 2, backward_step, 0)

    phase("small_rs")
    for copy in small_rs:
        copy.wait_recv()
    total = sm_all[dp]
    for k in range(n_dp - 1):
        total = total + sm_in[k]
    sm_ya[y] = total[:2]
    sm_zb[z] = total[2:]
    small_1 = []
    for k in ORDER:
        small_1.append(send(sm_ya.at[y], sm_ya.at[y], at_y[k]))
        small_1.append(send(sm_zb.at[z], sm_zb.at[z], at_z[k]))

    phase("rs2_wait")
    for copy in second_a + second_b:
        copy.wait_recv()
    fin_a[y, z] = t_a[z] + added([rt_a[k] for k in range(SIDE - 1)])
    fin_b[z, y] = t_b[y] + added([rt_b[k] for k in range(SIDE - 1)])
    phase("ag1_issue")
    along_a = {k: send(fin_a.at[y, z], fin_a.at[y, z], at_z[k]) for k in ORDER}
    along_b = {k: send(fin_b.at[z, y], fin_b.at[z, y], at_y[k]) for k in ORDER}

    across = {k: counter[0] + k - 1 for k in range(1, SIDE)}
    counter[0] += 2 * (SIDE - 1)

    def pass_on(a_z, b_y):
        for k in ORDER:
            tile = fin_a.at[y, a_z]
            remote(tile, tile, at_y[k], across[k]).start()
            tile = fin_b.at[z, b_y]
            remote(tile, tile, at_z[k], across[k] + SIDE - 1).start()

    pass_on(z, y)
    phase("backward2")
    lax.fori_loop(n_tiles // 2, n_tiles, backward_step, 0)
    stores = [local(gv_ref, gv_out), local(gg_ref, gg_out)]

    phase("small_1")
    for copy in small_1:
        copy.wait_recv()
    sm_za[z] = added([sm_ya[k] for k in range(SIDE)])
    sm_yb[y] = added([sm_zb[k] for k in range(SIDE)])
    small_2 = []
    for k in ORDER:
        small_2.append(send(sm_za.at[z], sm_za.at[z], at_z[k]))
        small_2.append(send(sm_yb.at[y], sm_yb.at[y], at_y[k]))

    phase("ag_pass")
    for k in NEAR_FIRST:
        along_a[k].wait_recv()
        along_b[k].wait_recv()
        pass_on((z + SIDE - k) % SIDE, (y + SIDE - k) % SIDE)

    phase("small_2")
    for copy in small_2:
        copy.wait_recv()
    sm_fin[dp, :2] = added([sm_za[k] for k in range(SIDE)])
    sm_fin[dp, 2:] = added([sm_yb[k] for k in range(SIDE)])
    small_ag = [send(sm_fin.at[dp], sm_fin.at[dp], at_dp[k]) for k in range(1, n_dp)]

    phase("ag2_wait")
    groups = []
    for k in range(1, SIDE):
        groups.append(remote(fin_a.at[y], fin_a.at[y], at_y[k], across[k]))
        groups.append(remote(fin_b.at[z], fin_b.at[z], at_z[k], across[k] + SIDE - 1))
    for group in groups:
        group.wait_recv()
    phase("assemble")
    width = channels // 2
    for r in range(SIDE):
        for t in range(SIDE):
            line = slice(r * part + (t // 2) * 8, r * part + (t // 2) * 8 + 8)
            c = (t % 2) * LANES
            gw_ref[line, c : c + LANES] = fin_a[r, t]
            gw_ref[line, width + c : width + c + LANES] = fin_b[r, t]
    stores.append(local(gw_ref, gw_out))

    phase("small_ag")
    for copy in small_ag:
        copy.wait_recv()
    for t in range(blocks * per_block):
        cb, rb = t // per_block, t % per_block
        lines[rb * 8 : rb * 8 + 8, lanes(cb)] = sm_fin[t // OWN_TILES, t % OWN_TILES]
    stores.append(local(lines, sm_out))
    phase("send_wait")
    for copy in started:
        copy.wait_send()
    for group in groups:
        group.wait_send()
    for copy in stores:
        copy.wait()
    phase(None)


def hand_out(gv, gg, gw, lines, gv_out, gg_out, gw_out, taps, gain, shift):
    n_taps = taps.shape[0]
    gv_out[...] = gv[...]
    gg_out[...] = gg[...]
    gw_out[...] = gw[...]
    taps[...] = lines[:n_taps]
    gain[...] = lines[n_taps : n_taps + 1]
    shift[...] = lines[n_taps + 1 : n_taps + 2]


def per_device(count, glu_value, glu_gate, cotangent, conv_weight, norm_gain, norm_shift, out_weight):
    value, gate, cot = glu_value[0], glu_gate[0], cotangent[0]
    rows, channels = value.shape
    n_taps = conv_weight.shape[0]
    features = out_weight.shape[0]
    blocks = channels // LANES
    part = features // SIDE
    n_dp = 2 * CHIPS
    scale = 1.0 / math.sqrt(rows * count)
    hbm = pl.BlockSpec(memory_space=pltpu.HBM)
    anywhere = pl.BlockSpec(memory_space=pl.ANY)
    vmem = pl.BlockSpec(memory_space=pltpu.VMEM)
    shape = jax.ShapeDtypeStruct
    buffer = pltpu.VMEM
    tile = (8, LANES)
    piece = (blocks, features, LANES)
    outs = pl.pallas_call(
        functools.partial(kernel, scale),
        out_shape=[
            pltpu.VMEM((rows, channels), BF16),
            pltpu.VMEM((rows, channels), BF16),
            pltpu.VMEM((features, channels), F32),
            pltpu.VMEM((SMALL, channels), F32),
        ],
        in_specs=[hbm] * 7,
        out_specs=[anywhere] * 4,
        scratch_shapes=[
            buffer((rows, channels), BF16),
            buffer((rows, channels), BF16),
            buffer(cot.shape, BF16),
            buffer((n_taps, channels), F32),
            buffer((1, channels), F32),
            buffer((1, channels), F32),
            buffer((features, channels), BF16),
            buffer((rows, channels), BF16),
            buffer((rows, channels), BF16),
            buffer((features, channels), F32),
            buffer((SMALL, channels), F32),
            buffer((HALO, channels), BF16),
            buffer((HALO, channels), BF16),
            buffer((blocks, rows + HALO, LANES), F32),
            buffer((blocks, rows, LANES), F32),
            buffer((rows, LANES), F32),
            buffer((blocks, rows, LANES), F32),
            buffer((rows, channels), F32),
            buffer((blocks, rows + HALO, LANES), F32),
            buffer((rows, channels), BF16),
            buffer((rows, channels), BF16),
            buffer((CHIPS, rows, features), BF16),
            buffer((n_dp * features, channels), BF16),
            buffer(piece, BF16),
            buffer(piece, BF16),
            buffer(piece, BF16),
            buffer(piece, BF16),
            buffer(piece, BF16),
            buffer(piece, BF16),
            buffer((features, channels), F32),
            buffer((features, channels), F32),
            buffer(piece, BF16),
            buffer((blocks, SIDE - 1, part, LANES), BF16),
            buffer((SIDE, *tile), F32),
            buffer((SIDE, *tile), F32),
            buffer((SIDE - 1, *tile), F32),
            buffer((SIDE - 1, *tile), F32),
            buffer((SIDE, SIDE, *tile), F32),
            buffer((SIDE, SIDE, *tile), F32),
            buffer((blocks, n_taps, *tile), F32),
            buffer((2, blocks, *tile), F32),
            buffer((n_dp, OWN_TILES, *tile), F32),
            buffer((n_dp - 1, OWN_TILES, *tile), F32),
            buffer((SIDE, 2, *tile), F32),
            buffer((SIDE, OWN_TILES - 2, *tile), F32),
            buffer((SIDE, 2, *tile), F32),
            buffer((SIDE, OWN_TILES - 2, *tile), F32),
            buffer((n_dp, OWN_TILES, *tile), F32),
            pltpu.SemaphoreType.DMA((COPIES,)),
            pltpu.SemaphoreType.DMA((COPIES,)),
            pltpu.SemaphoreType.DMA((16,)),
        ],
        compiler_params=pltpu.CompilerParams(
            collective_id=0, has_side_effects=True, vmem_limit_bytes=62 * 2**20
        ),
        name="backward",
    )(value, gate, cot, conv_weight, norm_gain[None], norm_shift[None], out_weight)
    grad_value, grad_gate, grad_weight, grad_taps, grad_gain, grad_shift = pl.pallas_call(
        hand_out,
        out_shape=[
            shape((rows, channels), BF16),
            shape((rows, channels), BF16),
            shape((features, channels), F32),
            shape((n_taps, channels), F32),
            shape((1, channels), F32),
            shape((1, channels), F32),
        ],
        in_specs=[vmem] * 4,
        out_specs=[vmem] * 6,
        compiler_params=pltpu.CompilerParams(vmem_limit_bytes=16 * 2**20),
        name="hand_out",
    )(*outs)
    return (
        grad_value[None], grad_gate[None], grad_weight,
        grad_taps, grad_gain.reshape(channels), grad_shift.reshape(channels),
    )


def solution(mesh):
    return jax.shard_map(
        functools.partial(per_device, mesh.size),
        mesh=mesh,
        in_specs=(
            P("dp", "sp", None), P("dp", "sp", None), P("dp", "sp", None),
            P(), P(), P(), P("dp", None),
        ),
        out_specs=(P("dp", "sp", None), P("dp", "sp", None), P("dp", None), P(), P(), P()),
        check_vma=False,
    )
```

```python
import functools
import math

import jax
import jax.numpy as jnp
from jax import lax
from jax.experimental import pallas as pl
from jax.experimental.pallas import tpu as pltpu
from jax.sharding import PartitionSpec as P

MESH = pl.DeviceIdType.MESH
F32 = jnp.float32
BF16 = jnp.bfloat16

EPS = 1e-06
LANES = 128
HALO = 32
TILE = 64
SIDE = 8
CHIPS = 4
RECEIVE_SEMS = 45
SEND_SEMS = 19
SMALL = 40
OWN_TILES = 3
ORDER = (4, 3, 5, 2, 6, 1, 7)
NEAR_FIRST = (1, 7, 2, 6, 3, 5, 4)


class Phases:
    def __init__(self):
        self.open = None

    def __call__(self, name):
        if self.open is not None:
            self.open.__exit__(None, None, None)
        self.open = None
        if name is not None:
            self.open = jax.named_scope(name)
            self.open.__enter__()


def sigmoid(x):
    return jax.nn.sigmoid(x)


def dot_t(a, b):
    return lax.dot_general(a, b, (((0,), (0,)), ((), ())), preferred_element_type=F32)


def added(terms):
    return functools.reduce(lambda a, b: a + b, terms)


def kernel(
    scale, v_hbm, g_hbm, cot_hbm, w_hbm, gain_hbm, shift_hbm, ow_hbm,
    gv_ref, gg_ref, gw_ref, taps_ref, grad_gain, grad_shift,
    v_ref, g_ref, cot_ref, w_ref, gain_ref, shift_ref, ow_ref,
    halo, halo_next, gated, normed, invs, dsil, ga, gcr, act, actp, cotp, wfull,
    far_st, opp_st, near_st, far_in, opp_in, near_in, near_own, own_part, gsum, cross_st, cross_own, cross_in, cross_sum, cross_x, spread_st, spread_in,
    t_a, t_b, rt_a, rt_b, fin_a, fin_b,
    taps, acc_gs, sm_all, sm_in, sm_ya, sm_zb, sm_za, sm_yb, sm_fin,
    send_sems, recv_sems, local_sems,
):
    phase = Phases()
    phase("start")
    rows, channels = v_ref.shape
    n_taps = w_ref.shape[0]
    blocks = channels // LANES
    features = ow_ref.shape[0]
    sp = lax.axis_index("sp")
    dp = lax.axis_index("dp")
    n_sp, n_dp = SIDE * SIDE, 2 * CHIPS
    z, y = sp // SIDE, sp % SIDE
    x, core = dp // 2, dp % 2
    step_x = 1 - 2 * core
    ahead_x = (x + CHIPS + step_x) % CHIPS
    behind_x = (x + CHIPS - step_x) % CHIPS
    far_x = (x + 2) % CHIPS

    other = {"sp": sp, "dp": 2 * x + (1 - core)}
    after = {"sp": (sp + 1) % n_sp, "dp": dp}
    before = {"sp": (sp + n_sp - 1) % n_sp, "dp": dp}
    at_y = {k: {"sp": z * SIDE + (y + k) % SIDE, "dp": dp} for k in range(1, SIDE)}
    at_z = {k: {"sp": ((z + k) % SIDE) * SIDE + y, "dp": dp} for k in range(1, SIDE)}
    at_dp = {k: {"sp": sp, "dp": (dp + k) % n_dp} for k in range(1, n_dp)}

    def chip(where):
        return {"sp": sp, "dp": 2 * where + core}

    barrier = pltpu.get_barrier_semaphore()
    peers = [after, before, *at_dp.values(), *at_y.values(), *at_z.values()]
    for peer in peers:
        pl.semaphore_signal(barrier, inc=1, device_id=peer, device_id_type=MESH)

    receive_ids, send_ids = {}, {}

    def remote(src, dst, device, got, sent):
        return pltpu.make_async_remote_copy(
            src_ref=src, dst_ref=dst,
            send_sem=send_sems.at[send_ids.setdefault(sent, len(send_ids))],
            recv_sem=recv_sems.at[receive_ids.setdefault(got, len(receive_ids))],
            device_id=device, device_id_type=MESH,
        )

    def send(src, dst, device, got, sent):
        remote(src, dst, device, got, sent).start()

    def arrived(got, size):
        remote(size, size, other, got, "w").wait_recv()

    def left(sent, size):
        remote(size, size, other, "pair_w", sent).wait_send()

    counter = [0]

    def local(src, dst):
        copy = pltpu.make_async_copy(src, dst, local_sems.at[counter[0]])
        counter[0] += 1
        copy.start()
        return copy

    loads = [
        local(v_hbm, v_ref), local(g_hbm, g_ref), local(ow_hbm, ow_ref), local(cot_hbm, cot_ref.at[pl.ds(0, rows), :]),
        local(w_hbm, w_ref), local(gain_hbm, gain_ref), local(shift_hbm, shift_ref),
    ]

    def lanes(cb):
        return slice(cb * LANES, (cb + 1) * LANES)

    def gate_tile(i, _):
        base = pl.multiple_of(i * TILE, TILE)
        for cb in range(blocks):
            v = v_ref[pl.ds(base, TILE), lanes(cb)].astype(F32)
            g = g_ref[pl.ds(base, TILE), lanes(cb)].astype(F32)
            gated[cb, pl.ds(base + HALO, TILE), :] = v * sigmoid(g)
        return 0

    phase("loads")
    loads[0].wait()
    loads[1].wait()
    phase("gate")
    lax.fori_loop(0, rows // TILE, gate_tile, 0)
    phase("loads2")
    for copy in loads[2:]:
        copy.wait()
    phase("barrier")
    pl.semaphore_wait(barrier, len(peers))
    phase("issue")

    send(v_ref.at[pl.ds(rows - HALO, HALO), :], halo.at[0], after, "halo", "halo")
    send(g_ref.at[pl.ds(rows - HALO, HALO), :], halo.at[1], after, "halo", "halo")
    send(v_ref.at[pl.ds(0, HALO), :], halo_next.at[0], before, "next", "next")
    send(g_ref.at[pl.ds(0, HALO), :], halo_next.at[1], before, "next", "next")
    next_rows = cot_ref.at[pl.ds(rows, HALO), :]

    def columns(owner_x, owner_core):
        return pl.ds(pl.multiple_of((2 * owner_x + owner_core) * features, features), features)

    def shard(owner_x, owner_core):
        return wfull.at[columns(owner_x, owner_core), :]

    parity = (y + z) % 2
    half_rows, quarter_rows = features // 2, features // 8

    def shard_half(owner_x, which):
        first = (2 * owner_x + core) * features + which * half_rows
        return wfull.at[pl.ds(pl.multiple_of(first, half_rows), half_rows), :]

    def shard_quarter(owner_x, i):
        first = (2 * owner_x + core) * features + parity * half_rows + i * quarter_rows
        return wfull.at[pl.ds(pl.multiple_of(first, quarter_rows), quarter_rows), :]

    own_half = ow_ref.at[pl.ds(pl.multiple_of(parity * half_rows, half_rows), half_rows), :]
    send(own_half, shard_half(x, parity), chip(ahead_x), "ahead", "w")
    send(own_half, shard_half(x, parity), chip(behind_x), "behind", "w")
    send(ow_ref, shard(x, core), other, "pair_w", "w")
    around = (at_y[1], at_y[SIDE - 1], at_z[1], at_z[SIDE - 1])

    def pass_half(owner_x, name):
        half_in = shard_half(owner_x, parity)
        for i in range(4):
            quarter = shard_quarter(owner_x, i)
            send(quarter, quarter, around[i], name, "w")
        send(half_in, half_in, other, "pair_w", "w")

    def pass_rest(owner_x, name):
        rest = shard_half(owner_x, 1 - parity)
        arrived(name, rest)
        send(rest, rest, other, "pair_w", "w")

    for k in range(CHIPS):
        send(cot_ref.at[pl.ds(0, rows), columns(k, 1 - core)], cotp.at[k], other, "cot", "cot")
    wfull[columns(x, core), :] = ow_ref[...]

    def conv_rows(base, size):
        for cb in range(blocks):
            acc = jnp.zeros((size, LANES), F32)
            for j in range(n_taps):
                tap = w_ref[j : j + 1, lanes(cb)]
                acc = acc + tap * gated[cb, pl.ds(base + (j + HALO - n_taps + 1), size), :]
            normed[cb, pl.ds(base, size), :] = acc

    def norm_rows(base, size, own=True):
        conv = [normed[cb, pl.ds(base, size), :] for cb in range(blocks)]
        mean = jnp.sum(added(conv), axis=-1, keepdims=True) * (1.0 / channels)
        centred = [c - mean for c in conv]
        var = jnp.sum(added([c * c for c in centred]), axis=-1, keepdims=True) * (1.0 / channels)
        inv = lax.rsqrt(var + EPS)
        invs[pl.ds(base, size), :] = jnp.broadcast_to(inv, (size, LANES))
        for cb in range(blocks):
            nrm = centred[cb] * inv
            pre = nrm * gain_ref[0:1, lanes(cb)] + shift_ref[0:1, lanes(cb)]
            sig = sigmoid(pre)
            normed[cb, pl.ds(base, size), :] = nrm
            if own:
                act[pl.ds(base, size), lanes(cb)] = (pre * sig).astype(BF16)
            dsil[cb, pl.ds(base, size), :] = sig * (1.0 + pre * (1.0 - sig))

    def over_tiles(first_tile, last_tile, step):
        def body(i, _):
            step(pl.multiple_of(i * TILE, TILE), TILE)
            return 0

        lax.fori_loop(first_tile, last_tile, body, 0)

    def forward(first_tile, last_tile):
        over_tiles(first_tile, last_tile, conv_rows)
        over_tiles(first_tile, last_tile, norm_rows)

    def send_act(first, last):
        lines = pl.ds(first * TILE, (last - first) * TILE)
        send(act.at[lines, :], actp.at[lines, :], other, "act", "act")

    n_tiles = rows // TILE
    phase("forward")
    forward(1, n_tiles // 2)
    send_act(1, n_tiles // 2)
    forward(n_tiles // 2, n_tiles)
    send_act(n_tiles // 2, n_tiles)
    phase("halo_wait")
    arrived("halo", halo)
    phase("forward0")
    inside = (sp > 0).astype(F32)
    for cb in range(blocks):
        v = halo[0, :, lanes(cb)].astype(F32)
        g = halo[1, :, lanes(cb)].astype(F32)
        gated[cb, pl.ds(0, HALO), :] = v * sigmoid(g) * inside
    forward(0, 1)
    send_act(0, 1)

    phase("w_wait1")
    arrived("ahead", shard_half(behind_x, parity))
    passed = shard_half(behind_x, parity)
    send(passed, passed, chip(ahead_x), "far", "w")
    pass_half(behind_x, "quarters_behind")
    arrived("behind", shard_half(ahead_x, parity))
    pass_half(ahead_x, "quarters_ahead")
    send(cot_ref.at[pl.ds(0, HALO), :], next_rows, before, "next_cot", "next_cot")

    phase("forward_next")
    arrived("next", halo_next)
    for cb in range(blocks):
        v = halo_next[0, :, lanes(cb)].astype(F32)
        g = halo_next[1, :, lanes(cb)].astype(F32)
        gated[cb, pl.ds(rows + HALO, HALO), :] = v * sigmoid(g)
    conv_rows(rows, HALO)
    norm_rows(rows, HALO, own=False)

    pieces, crossing = (0, 1), (2, 3)
    part = features // SIDE
    mine, around_all = (y, z, y, z), (at_y, at_z, at_y, at_z)

    def chunk_of(where):
        return pl.ds(pl.multiple_of(where * part, part), part)

    def own_product(owner_x):
        return dot_t(cot_ref[pl.ds(0, rows), columns(owner_x, core)], act[...])

    def other_product(owner_x):
        return dot_t(cotp[owner_x], actp[...])

    phase("product0")
    own_part[0] = own_product(far_x)
    own_part[1] = own_product(behind_x)
    phase("act_wait")
    arrived("cot", cotp)
    arrived("act", actp)
    phase("product")
    def kept(owner_x, value, store):
        rounded = value.astype(BF16)
        for p in crossing:
            cross_own[p - 2, owner_x] = value[:, lanes(p)]
            cross_st[p - 2, owner_x] = rounded[:, lanes(p)]
        for p in pieces:
            store[p] = (value if store.dtype == F32 else rounded)[:, lanes(p)]

    kept(far_x, own_part[0] + other_product(far_x), far_st)
    for p in pieces:
        send(far_st.at[p], far_in.at[p], chip(ahead_x), ("far", p), "far")
    kept(behind_x, own_part[1] + other_product(behind_x), opp_st)
    for p in pieces:
        send(opp_st.at[p], opp_in.at[p], chip(behind_x), ("opp", p), "opp")
    kept(ahead_x, own_product(ahead_x) + other_product(ahead_x), near_own)
    kept(x, own_product(x) + other_product(x), gsum)
    def relay(p):
        arrived(("far", p), far_in.at[p])
        near_st[p] = (near_own[p] + far_in[p].astype(F32)).astype(BF16)
        send(near_st.at[p], near_in.at[p], chip(ahead_x), ("near", p), "near")

    phase("w_rest0")
    pass_rest(behind_x, "quarters_behind")
    passed_rest = shard_half(behind_x, 1 - parity)
    send(passed_rest, passed_rest, chip(ahead_x), "far_rest", "w")
    phase("w_rest1")
    pass_rest(ahead_x, "quarters_ahead")
    for k in ORDER:
        for p in crossing:
            source = cross_st.at[p - 2, :, chunk_of((mine[p] + k) % SIDE), :]
            send(source, cross_in.at[p - 2, k - 1], around_all[p][k], "cross", "cross")
    phase("w_wait2")
    for name, which in (("far", parity), ("far_rest", 1 - parity)):
        far_half = shard_half(far_x, which)
        arrived(name, far_half)
        send(far_half, far_half, other, "pair_w", "w")
    phase("relay0")
    relay(0)
    relay(1)
    phase("w_wait4")
    arrived("pair_w", wfull.at[pl.ds(0, CHIPS * features), :])

    phase("matmul")
    arrived("next_cot", next_rows)
    half = (rows + HALO) // 2

    def matmul_step(i, _):
        base = pl.multiple_of(i * half, 16)
        ga[pl.ds(base, half), :] = jnp.dot(
            cot_ref[pl.ds(base, half), :], wfull[...], preferred_element_type=F32
        )
        return 0

    lax.fori_loop(0, 2, matmul_step, 0)
    phase("grad")
    acc_gs[...] = jnp.zeros_like(acc_gs)
    taps[...] = jnp.zeros_like(taps)

    def fold(a):
        return a.reshape(TILE // 8, 8, LANES).sum(axis=0)

    def grad_rows(base, size, own=True):
        grads, norms = [], []
        for cb in range(blocks):
            gpre = ga[pl.ds(base, size), lanes(cb)] * dsil[cb, pl.ds(base, size), :]
            nrm = normed[cb, pl.ds(base, size), :]
            if own:
                acc_gs[0, cb] = acc_gs[0, cb] + fold(gpre * nrm)
                acc_gs[1, cb] = acc_gs[1, cb] + fold(gpre)
            grads.append(gpre * gain_ref[0:1, lanes(cb)])
            norms.append(nrm)
        mean = jnp.sum(added(grads), axis=-1, keepdims=True) * (1.0 / channels)
        along = added([a * b for a, b in zip(grads, norms)])
        mean_along = jnp.sum(along, axis=-1, keepdims=True) * (1.0 / channels)
        inv = invs[pl.ds(base, size), :]
        for cb in range(blocks):
            gcr[cb, pl.ds(base, size), :] = inv * (grads[cb] - mean - norms[cb] * mean_along)

    over_tiles(0, n_tiles, grad_rows)
    grad_rows(rows, HALO, own=False)
    beyond = (sp < n_sp - 1).astype(F32)
    for cb in range(blocks):
        gcr[cb, pl.ds(rows, HALO), :] = gcr[cb, pl.ds(rows, HALO), :] * beyond

    def chip_sum(p):
        arrived(("near", p), near_in.at[p])
        arrived(("opp", p), opp_in.at[p])
        total = gsum[p] + near_in[p].astype(F32) + opp_in[p].astype(F32)
        gsum[p] = total
        spread_st[p] = total.astype(BF16)
        for k in ORDER:
            source = spread_st.at[p, chunk_of((mine[p] + k) % SIDE), :]
            send(source, spread_in.at[p, k - 1], around_all[p][k], "spread", "spread")

    phase("chip_sum")
    for p in pieces:
        chip_sum(p)

    def taps_step(i, _):
        base = pl.multiple_of(i * TILE, TILE)
        for cb in range(blocks):
            own = gated[cb, pl.ds(base + HALO, TILE), :]
            for j in range(n_taps):
                shifted = gcr[cb, pl.ds(base + (n_taps - 1 - j), TILE), :]
                taps[cb, j] = taps[cb, j] + fold(own * shifted)
        return 0

    phase("taps1")
    lax.fori_loop(0, n_tiles // 2, taps_step, 0)
    phase("cross_wait")
    arrived("cross", cross_in)
    for p in crossing:
        for owner in range(CHIPS):
            total = cross_own[p - 2, owner, chunk_of(mine[p]), :]
            for k in range(SIDE - 1):
                total = total + cross_in[p - 2, k, owner].astype(F32)
            cross_sum[p - 2, owner] = total
        for k in (2, 1, 3):
            to = (x + k) % CHIPS
            send(cross_sum.at[p - 2, to], cross_x.at[p - 2, k - 1], chip(to), "cross_x", "cross_x")
    phase("taps2")
    lax.fori_loop(n_tiles // 2, n_tiles, taps_step, 0)

    phase("small_fold")
    per_block = SMALL // 8
    row_ids = lax.broadcasted_iota(jnp.int32, (8, LANES), 0)
    for t in range(n_dp * OWN_TILES):
        cb, rb = t // per_block, t % per_block
        tile = jnp.zeros((8, LANES), F32)
        if cb < blocks:
            for r in range(8):
                j = rb * 8 + r
                if j < n_taps:
                    line = taps[cb, j]
                elif j < n_taps + 2:
                    line = acc_gs[j - n_taps, cb]
                else:
                    continue
                line = jnp.sum(line, axis=0, keepdims=True) * scale
                tile = jnp.where(row_ids == r, line, tile)
        sm_all[t // OWN_TILES, t % OWN_TILES] = tile
    for k in range(1, n_dp):
        send(sm_all.at[(dp + k) % n_dp], sm_in.at[k - 1], at_dp[k], "small_0", "small_0")

    def backward_step(i, _):
        base = pl.multiple_of(i * TILE, TILE)
        for cb in range(blocks):
            acc = jnp.zeros((TILE, LANES), F32)
            for j in range(n_taps):
                tap = w_ref[j : j + 1, lanes(cb)]
                acc = acc + tap * gcr[cb, pl.ds(base + (n_taps - 1 - j), TILE), :]
            v = v_ref[pl.ds(base, TILE), lanes(cb)].astype(F32)
            sig = sigmoid(g_ref[pl.ds(base, TILE), lanes(cb)].astype(F32))
            gs = acc * sig
            gv_ref[pl.ds(base, TILE), lanes(cb)] = gs.astype(BF16)
            gg_ref[pl.ds(base, TILE), lanes(cb)] = (gs * v * (1.0 - sig)).astype(BF16)
        return 0

    first = pl.ds(0, SIDE - 1)
    early, late = n_tiles // 2, n_tiles - 1

    phase("backward1")
    lax.fori_loop(0, early, backward_step, 0)

    phase("rs1_wait")
    arrived("spread", spread_in)
    arrived("cross_x", cross_x)
    phase("rs1_sum")

    def first_sum(p, t_ref):
        summed = gsum[p, chunk_of(mine[p]), :]
        for k in range(SIDE - 1):
            summed = summed + spread_in[p, k].astype(F32)
        crossed = cross_sum[p, x]
        for k in range(CHIPS - 1):
            crossed = crossed + cross_x[p, k]
        for c, total in enumerate((summed, crossed)):
            for r in range(part // 8):
                t_ref[2 * r + c] = total[r * 8 : r * 8 + 8, :] * scale

    first_sum(0, t_a)
    first_sum(1, t_b)
    for k in ORDER:
        send(t_a.at[(z + k) % SIDE], rt_a.at[k - 1], at_z[k], "second_a", "tiles")
        send(t_b.at[(y + k) % SIDE], rt_b.at[k - 1], at_y[k], "second_b", "tiles")

    phase("backward2")
    lax.fori_loop(early, late, backward_step, 0)

    phase("small_0")
    arrived("small_0", sm_in)
    total = sm_all[dp]
    for k in range(n_dp - 1):
        total = total + sm_in[k]
    sm_ya[y] = total[:2]
    sm_zb[z] = total[2:]
    for k in ORDER:
        send(sm_ya.at[y], sm_ya.at[y], at_y[k], "small_1a", "small_1")
        send(sm_zb.at[z], sm_zb.at[z], at_z[k], "small_1b", "small_1")

    phase("backward3")
    lax.fori_loop(late, n_tiles, backward_step, 0)

    phase("rs2_wait")
    arrived("second_a", rt_a)
    arrived("second_b", rt_b)
    fin_a[y, z] = t_a[z] + added([rt_a[k] for k in range(SIDE - 1)])
    fin_b[z, y] = t_b[y] + added([rt_b[k] for k in range(SIDE - 1)])
    for k in ORDER:
        send(fin_a.at[y, z], fin_a.at[y, z], at_z[k], ("along_a", k), "tiles")
        send(fin_b.at[z, y], fin_b.at[z, y], at_y[k], ("along_b", k), "tiles")

    def pass_on(a_z, b_y):
        for k in ORDER:
            send(fin_a.at[y, a_z], fin_a.at[y, a_z], at_y[k], "across_a", "across_a")
            send(fin_b.at[z, b_y], fin_b.at[z, b_y], at_z[k], "across_b", "across_b")

    pass_on(z, y)

    phase("small_1")
    arrived("small_1a", sm_ya.at[first])
    arrived("small_1b", sm_zb.at[first])
    sm_za[z] = added([sm_ya[k] for k in range(SIDE)])
    sm_yb[y] = added([sm_zb[k] for k in range(SIDE)])
    for k in ORDER:
        send(sm_za.at[z], sm_za.at[z], at_z[k], "small_2a", "small_2")
        send(sm_yb.at[y], sm_yb.at[y], at_y[k], "small_2b", "small_2")

    phase("ag_pass")
    for k in NEAR_FIRST:
        arrived(("along_a", k), rt_a.at[0])
        arrived(("along_b", k), rt_b.at[0])
        pass_on((z + SIDE - k) % SIDE, (y + SIDE - k) % SIDE)

    phase("small_2")
    arrived("small_2a", sm_za.at[first])
    arrived("small_2b", sm_yb.at[first])
    sm_fin[dp, :2] = added([sm_za[k] for k in range(SIDE)])
    sm_fin[dp, 2:] = added([sm_yb[k] for k in range(SIDE)])
    for k in range(1, n_dp):
        send(sm_fin.at[dp], sm_fin.at[dp], at_dp[k], "small_3", "small_3")

    phase("ag2_wait")
    arrived("across_a", fin_a.at[first])
    arrived("across_b", fin_b.at[first])
    phase("assemble")
    for r in range(SIDE):
        for t in range(SIDE):
            line = slice(r * part + (t // 2) * 8, r * part + (t // 2) * 8 + 8)
            gw_ref[line, lanes(2 * (t % 2))] = fin_a[r, t]
            gw_ref[line, lanes(2 * (t % 2) + 1)] = fin_b[r, t]

    phase("small_3")
    arrived("small_3", sm_fin.at[pl.ds(0, n_dp - 1)])
    for t in range(blocks * per_block):
        cb, rb = t // per_block, t % per_block
        tile = sm_fin[t // OWN_TILES, t % OWN_TILES]
        for first_row, count, out in (
            (0, n_taps, taps_ref), (n_taps, 1, grad_gain), (n_taps + 1, 1, grad_shift)
        ):
            low, high = max(first_row, rb * 8), min(first_row + count, rb * 8 + 8)
            if low < high:
                out[low - first_row : high - first_row, lanes(cb)] = tile[low - rb * 8 : high - rb * 8]
    phase("send_wait")
    left("w", wfull.at[pl.ds(0, 7 * features), :])
    left("cot", cotp)
    left("act", actp)
    left("halo", halo)
    left("next", halo_next)
    left("next_cot", next_rows)
    left("far", far_in)
    left("opp", opp_in)
    left("near", near_in)
    left("spread", spread_in)
    left("cross", cross_in)
    left("cross_x", cross_x)
    left("tiles", fin_a.at[first, pl.ds(0, 4)])
    left("across_a", fin_a.at[first])
    left("across_b", fin_b.at[first])
    for i in range(4):
        left(f"small_{i}", sm_in)
    phase(None)
    assert len(send_ids) == SEND_SEMS and len(receive_ids) == RECEIVE_SEMS


def hand_out(*refs):
    sources, targets, sems = refs[:6], refs[6:12], refs[12]
    copies = [
        pltpu.make_async_copy(a, b, sems.at[i]) for i, (a, b) in enumerate(zip(sources, targets))
    ]
    for copy in copies:
        copy.start()
    for copy in copies:
        copy.wait()


def per_device(count, glu_value, glu_gate, cotangent, conv_weight, norm_gain, norm_shift, out_weight):
    value, gate, cot = glu_value[0], glu_gate[0], cotangent[0]
    rows, channels = value.shape
    n_taps = conv_weight.shape[0]
    features = out_weight.shape[0]
    blocks = channels // LANES
    part = features // SIDE
    n_dp = 2 * CHIPS
    scale = 1.0 / math.sqrt(rows * count)
    hbm = pl.BlockSpec(memory_space=pltpu.HBM)
    anywhere = pl.BlockSpec(memory_space=pl.ANY)
    vmem = pl.BlockSpec(memory_space=pltpu.VMEM)
    shape = jax.ShapeDtypeStruct
    buffer = pltpu.VMEM
    tile = (8, LANES)
    piece = (2, features, LANES)
    outs = pl.pallas_call(
        functools.partial(kernel, scale),
        out_shape=[
            pltpu.VMEM((rows, channels), BF16),
            pltpu.VMEM((rows, channels), BF16),
            pltpu.VMEM((features, channels), F32),
            pltpu.VMEM((n_taps, channels), F32),
            pltpu.VMEM((1, channels), F32),
            pltpu.VMEM((1, channels), F32),
        ],
        in_specs=[hbm] * 7,
        out_specs=[vmem] * 6,
        scratch_shapes=[
            buffer((rows, channels), BF16),
            buffer((rows, channels), BF16),
            buffer((rows + HALO, cot.shape[1]), BF16),
            buffer((n_taps, channels), F32),
            buffer((1, channels), F32),
            buffer((1, channels), F32),
            buffer((features, channels), BF16),
            buffer((2, HALO, channels), BF16),
            buffer((2, HALO, channels), BF16),
            buffer((blocks, rows + 2 * HALO, LANES), F32),
            buffer((blocks, rows + HALO, LANES), F32),
            buffer((rows + HALO, LANES), F32),
            buffer((blocks, rows + HALO, LANES), F32),
            buffer((rows + HALO, channels), F32),
            buffer((blocks, rows + HALO, LANES), F32),
            buffer((rows, channels), BF16),
            buffer((rows, channels), BF16),
            buffer((CHIPS, rows, features), BF16),
            buffer((n_dp * features, channels), BF16),
            buffer(piece, BF16),
            buffer(piece, BF16),
            buffer(piece, BF16),
            buffer(piece, BF16),
            buffer(piece, BF16),
            buffer(piece, BF16),
            buffer(piece, F32),
            buffer((2, features, channels), F32),
            buffer(piece, F32),
            buffer((2, CHIPS, features, LANES), BF16),
            buffer((2, CHIPS, features, LANES), F32),
            buffer((2, SIDE - 1, CHIPS, part, LANES), BF16),
            buffer((2, CHIPS, part, LANES), F32),
            buffer((2, CHIPS - 1, part, LANES), F32),
            buffer(piece, BF16),
            buffer((2, SIDE - 1, part, LANES), BF16),
            buffer((SIDE, *tile), F32),
            buffer((SIDE, *tile), F32),
            buffer((SIDE - 1, *tile), F32),
            buffer((SIDE - 1, *tile), F32),
            buffer((SIDE, SIDE, *tile), F32),
            buffer((SIDE, SIDE, *tile), F32),
            buffer((blocks, n_taps, *tile), F32),
            buffer((2, blocks, *tile), F32),
            buffer((n_dp, OWN_TILES, *tile), F32),
            buffer((n_dp - 1, OWN_TILES, *tile), F32),
            buffer((SIDE, 2, *tile), F32),
            buffer((SIDE, OWN_TILES - 2, *tile), F32),
            buffer((SIDE, 2, *tile), F32),
            buffer((SIDE, OWN_TILES - 2, *tile), F32),
            buffer((n_dp, OWN_TILES, *tile), F32),
            pltpu.SemaphoreType.DMA((SEND_SEMS,)),
            pltpu.SemaphoreType.DMA((RECEIVE_SEMS,)),
            pltpu.SemaphoreType.DMA((7,)),
        ],
        compiler_params=pltpu.CompilerParams(
            collective_id=0, has_side_effects=True, vmem_limit_bytes=62 * 2**20
        ),
        name="backward",
    )(value, gate, cot, conv_weight, norm_gain[None], norm_shift[None], out_weight)
    grad_value, grad_gate, grad_weight, grad_taps, grad_gain, grad_shift = pl.pallas_call(
        hand_out,
        out_shape=[
            shape((rows, channels), BF16),
            shape((rows, channels), BF16),
            shape((features, channels), F32),
            shape((n_taps, channels), F32),
            shape((1, channels), F32),
            shape((1, channels), F32),
        ],
        in_specs=[vmem] * 6,
        out_specs=[anywhere] * 6,
        scratch_shapes=[pltpu.SemaphoreType.DMA((6,))],
        compiler_params=pltpu.CompilerParams(vmem_limit_bytes=16 * 2**20),
        name="hand_out",
    )(*outs)
    return (
        grad_value[None], grad_gate[None], grad_weight,
        grad_taps, grad_gain.reshape(channels), grad_shift.reshape(channels),
    )


def solution(mesh):
    return jax.shard_map(
        functools.partial(per_device, mesh.size),
        mesh=mesh,
        in_specs=(
            P("dp", "sp", None), P("dp", "sp", None), P("dp", "sp", None),
            P(), P(), P(), P("dp", None),
        ),
        out_specs=(P("dp", "sp", None), P("dp", "sp", None), P("dp", None), P(), P(), P()),
        check_vma=False,
    )
```

```python
import functools
import math

import jax
import jax.numpy as jnp
from jax import lax
from jax.experimental import pallas as pl
from jax.experimental.pallas import tpu as pltpu
from jax.sharding import PartitionSpec as P

MESH = pl.DeviceIdType.MESH
F32 = jnp.float32
BF16 = jnp.bfloat16

EPS = 1e-06
LANES = 128
HALO = 32
TILE = 64
SIDE = 8
CHIPS = 4
RECEIVE_SEMS = 45
SEND_SEMS = 19
SMALL = 40
OWN_TILES = 3
ORDER = (4, 3, 5, 2, 6, 1, 7)
NEAR_FIRST = (1, 7, 2, 6, 3, 5, 4)


class Phases:
    def __init__(self):
        self.open = None

    def __call__(self, name):
        if self.open is not None:
            self.open.__exit__(None, None, None)
        self.open = None
        if name is not None:
            self.open = jax.named_scope(name)
            self.open.__enter__()


def sigmoid(x):
    return jax.nn.sigmoid(x)


def dot_t(a, b):
    return lax.dot_general(a, b, (((0,), (0,)), ((), ())), preferred_element_type=F32)


def added(terms):
    return functools.reduce(lambda a, b: a + b, terms)


def kernel(
    scale, v_hbm, g_hbm, cot_hbm, w_hbm, gain_hbm, shift_hbm, ow_hbm,
    gv_ref, gg_ref, gw_ref, taps_ref, grad_gain, grad_shift,
    v_ref, g_ref, cot_ref, w_ref, gain_ref, shift_ref, ow_ref,
    halo, halo_next, gated, normed, invs, dsil, ga, gcr, act, actp, cotp, wfull,
    far_st, opp_st, near_st, far_in, opp_in, near_in, near_own, own_part, gsum, cross_st, cross_own, cross_in, cross_sum, cross_x, spread_st, spread_in,
    t_a, t_b, rt_a, rt_b, fin_a, fin_b,
    taps, acc_gs, sm_all, sm_in, sm_ya, sm_zb, sm_za, sm_yb, sm_fin,
    send_sems, recv_sems, local_sems,
):
    phase = Phases()
    phase("start")
    rows, channels = v_ref.shape
    n_taps = w_ref.shape[0]
    blocks = channels // LANES
    features = ow_ref.shape[0]
    sp = lax.axis_index("sp")
    dp = lax.axis_index("dp")
    n_sp, n_dp = SIDE * SIDE, 2 * CHIPS
    z, y = sp // SIDE, sp % SIDE
    x, core = dp // 2, dp % 2
    step_x = 1 - 2 * core
    ahead_x = (x + CHIPS + step_x) % CHIPS
    behind_x = (x + CHIPS - step_x) % CHIPS
    far_x = (x + 2) % CHIPS

    other = {"sp": sp, "dp": 2 * x + (1 - core)}
    after = {"sp": (sp + 1) % n_sp, "dp": dp}
    before = {"sp": (sp + n_sp - 1) % n_sp, "dp": dp}
    at_y = {k: {"sp": z * SIDE + (y + k) % SIDE, "dp": dp} for k in range(1, SIDE)}
    at_z = {k: {"sp": ((z + k) % SIDE) * SIDE + y, "dp": dp} for k in range(1, SIDE)}
    at_dp = {k: {"sp": sp, "dp": (dp + k) % n_dp} for k in range(1, n_dp)}

    def chip(where):
        return {"sp": sp, "dp": 2 * where + core}

    barrier = pltpu.get_barrier_semaphore()
    peers = [at[k] for k in ORDER for at in (at_y, at_z)]
    peers += [after, before, *at_dp.values()]
    for peer in peers:
        pl.semaphore_signal(barrier, inc=1, device_id=peer, device_id_type=MESH)

    receive_ids, send_ids = {}, {}

    def remote(src, dst, device, got, sent):
        return pltpu.make_async_remote_copy(
            src_ref=src, dst_ref=dst,
            send_sem=send_sems.at[send_ids.setdefault(sent, len(send_ids))],
            recv_sem=recv_sems.at[receive_ids.setdefault(got, len(receive_ids))],
            device_id=device, device_id_type=MESH,
        )

    def send(src, dst, device, got, sent):
        remote(src, dst, device, got, sent).start()

    def arrived(got, size):
        remote(size, size, other, got, "w").wait_recv()

    def left(sent, size):
        remote(size, size, other, "pair_w", sent).wait_send()

    counter = [0]

    def local(src, dst):
        copy = pltpu.make_async_copy(src, dst, local_sems.at[counter[0]])
        counter[0] += 1
        copy.start()
        return copy

    loads = [
        local(v_hbm, v_ref), local(g_hbm, g_ref), local(ow_hbm, ow_ref), local(cot_hbm, cot_ref.at[pl.ds(0, rows), :]),
        local(w_hbm, w_ref), local(gain_hbm, gain_ref), local(shift_hbm, shift_ref),
    ]

    def lanes(cb):
        return slice(cb * LANES, (cb + 1) * LANES)

    def gate_tile(i, _):
        base = pl.multiple_of(i * TILE, TILE)
        for cb in range(blocks):
            v = v_ref[pl.ds(base, TILE), lanes(cb)].astype(F32)
            g = g_ref[pl.ds(base, TILE), lanes(cb)].astype(F32)
            gated[cb, pl.ds(base + HALO, TILE), :] = v * sigmoid(g)
        return 0

    phase("loads")
    loads[0].wait()
    loads[1].wait()
    phase("gate")
    lax.fori_loop(0, rows // TILE, gate_tile, 0)
    phase("loads2")
    for copy in loads[2:]:
        copy.wait()
    def conv_rows(base, size):
        for cb in range(blocks):
            acc = jnp.zeros((size, LANES), F32)
            for j in range(n_taps):
                tap = w_ref[j : j + 1, lanes(cb)]
                acc = acc + tap * gated[cb, pl.ds(base + (j + HALO - n_taps + 1), size), :]
            normed[cb, pl.ds(base, size), :] = acc

    def norm_rows(base, size, own=True):
        conv = [normed[cb, pl.ds(base, size), :] for cb in range(blocks)]
        mean = jnp.sum(added(conv), axis=-1, keepdims=True) * (1.0 / channels)
        centred = [c - mean for c in conv]
        var = jnp.sum(added([c * c for c in centred]), axis=-1, keepdims=True) * (1.0 / channels)
        inv = lax.rsqrt(var + EPS)
        invs[pl.ds(base, size), :] = jnp.broadcast_to(inv, (size, LANES))
        for cb in range(blocks):
            nrm = centred[cb] * inv
            pre = nrm * gain_ref[0:1, lanes(cb)] + shift_ref[0:1, lanes(cb)]
            sig = sigmoid(pre)
            normed[cb, pl.ds(base, size), :] = nrm
            if own:
                act[pl.ds(base, size), lanes(cb)] = (pre * sig).astype(BF16)
            dsil[cb, pl.ds(base, size), :] = sig * (1.0 + pre * (1.0 - sig))

    def over_tiles(first_tile, last_tile, step):
        def body(i, _):
            step(pl.multiple_of(i * TILE, TILE), TILE)
            return 0

        lax.fori_loop(first_tile, last_tile, body, 0)

    def forward(first_tile, last_tile):
        over_tiles(first_tile, last_tile, conv_rows)
        over_tiles(first_tile, last_tile, norm_rows)

    n_tiles = rows // TILE
    phase("forward_a")
    forward(1, 3)
    phase("barrier")
    pl.semaphore_wait(barrier, len(peers))
    phase("issue")

    send(v_ref.at[pl.ds(rows - HALO, HALO), :], halo.at[0], after, "halo", "halo")
    send(g_ref.at[pl.ds(rows - HALO, HALO), :], halo.at[1], after, "halo", "halo")
    send(v_ref.at[pl.ds(0, HALO), :], halo_next.at[0], before, "next", "next")
    send(g_ref.at[pl.ds(0, HALO), :], halo_next.at[1], before, "next", "next")
    next_rows = cot_ref.at[pl.ds(rows, HALO), :]

    def columns(owner_x, owner_core):
        return pl.ds(pl.multiple_of((2 * owner_x + owner_core) * features, features), features)

    def shard(owner_x, owner_core):
        return wfull.at[columns(owner_x, owner_core), :]

    half_rows = features // 2

    def shard_half(owner_x, which):
        first = (2 * owner_x + core) * features + which * half_rows
        return wfull.at[pl.ds(pl.multiple_of(first, half_rows), half_rows), :]

    for h in range(2):
        own_half = ow_ref.at[pl.ds(h * half_rows, half_rows), :]
        send(own_half, shard_half(x, h), chip(ahead_x), ("ahead", h), "w")
        send(own_half, shard_half(x, h), chip(behind_x), ("behind", h), "w")
    send(ow_ref, shard(x, core), other, "pair_w", "w")

    def to_other(half):
        send(half, half, other, "pair_w", "w")

    def pass_half(h):
        half = shard_half(behind_x, h)
        arrived(("ahead", h), half)
        send(half, half, chip(ahead_x), ("far_w", h), "w")
        to_other(half)
        half = shard_half(ahead_x, h)
        arrived(("behind", h), half)
        to_other(half)

    for k in range(CHIPS):
        send(cot_ref.at[pl.ds(0, rows), columns(k, 1 - core)], cotp.at[k], other, "cot", "cot")
    wfull[columns(x, core), :] = ow_ref[...]

    def send_act(first, last):
        lines = pl.ds(first * TILE, (last - first) * TILE)
        send(act.at[lines, :], actp.at[lines, :], other, "act", "act")

    phase("forward")
    forward(3, n_tiles // 2)
    send_act(1, n_tiles // 2)
    forward(n_tiles // 2, n_tiles)
    send_act(n_tiles // 2, n_tiles)
    phase("halo_wait")
    arrived("halo", halo)
    phase("forward0")
    inside = (sp > 0).astype(F32)
    for cb in range(blocks):
        v = halo[0, :, lanes(cb)].astype(F32)
        g = halo[1, :, lanes(cb)].astype(F32)
        gated[cb, pl.ds(0, HALO), :] = v * sigmoid(g) * inside
    forward(0, 1)
    send_act(0, 1)

    phase("w_wait1")
    pass_half(0)
    send(cot_ref.at[pl.ds(0, HALO), :], next_rows, before, "next_cot", "next_cot")

    phase("forward_next")
    arrived("next", halo_next)
    for cb in range(blocks):
        v = halo_next[0, :, lanes(cb)].astype(F32)
        g = halo_next[1, :, lanes(cb)].astype(F32)
        gated[cb, pl.ds(rows + HALO, HALO), :] = v * sigmoid(g)
    conv_rows(rows, HALO)
    norm_rows(rows, HALO, own=False)

    pieces, crossing = (0, 1), (2, 3)
    part = features // SIDE
    mine, around_all = (y, z, y, z), (at_y, at_z, at_y, at_z)

    def chunk_of(where):
        return pl.ds(pl.multiple_of(where * part, part), part)

    def own_product(owner_x):
        return dot_t(cot_ref[pl.ds(0, rows), columns(owner_x, core)], act[...])

    def other_product(owner_x):
        return dot_t(cotp[owner_x], actp[...])

    phase("product0")
    own_part[0] = own_product(far_x)
    own_part[1] = own_product(behind_x)
    phase("act_wait")
    arrived("cot", cotp)
    arrived("act", actp)
    phase("product")
    def kept(owner_x, value, store):
        rounded = value.astype(BF16)
        for p in crossing:
            cross_own[p - 2, owner_x] = value[:, lanes(p)]
            cross_st[p - 2, owner_x] = rounded[:, lanes(p)]
        for p in pieces:
            store[p] = (value if store.dtype == F32 else rounded)[:, lanes(p)]

    kept(far_x, own_part[0] + other_product(far_x), far_st)
    for p in pieces:
        send(far_st.at[p], far_in.at[p], chip(ahead_x), ("far", p), "far")
    kept(behind_x, own_part[1] + other_product(behind_x), opp_st)
    for p in pieces:
        send(opp_st.at[p], opp_in.at[p], chip(behind_x), ("opp", p), "opp")
    kept(ahead_x, own_product(ahead_x) + other_product(ahead_x), near_own)
    kept(x, own_product(x) + other_product(x), gsum)
    def relay(p):
        arrived(("far", p), far_in.at[p])
        near_st[p] = (near_own[p] + far_in[p].astype(F32)).astype(BF16)
        send(near_st.at[p], near_in.at[p], chip(ahead_x), ("near", p), "near")

    for k in ORDER:
        for p in crossing:
            source = cross_st.at[p - 2, :, chunk_of((mine[p] + k) % SIDE), :]
            send(source, cross_in.at[p - 2, k - 1], around_all[p][k], "cross", "cross")
    phase("w_wait1b")
    pass_half(1)
    phase("relay0")
    relay(0)
    relay(1)
    phase("w_wait2")
    for h in range(2):
        arrived(("far_w", h), shard_half(far_x, h))
        to_other(shard_half(far_x, h))
    phase("w_wait4")
    arrived("pair_w", wfull.at[pl.ds(0, CHIPS * features), :])

    phase("matmul")
    arrived("next_cot", next_rows)
    half = (rows + HALO) // 2

    def matmul_step(i, _):
        base = pl.multiple_of(i * half, 16)
        ga[pl.ds(base, half), :] = jnp.dot(
            cot_ref[pl.ds(base, half), :], wfull[...], preferred_element_type=F32
        )
        return 0

    lax.fori_loop(0, 2, matmul_step, 0)
    phase("grad")
    acc_gs[...] = jnp.zeros_like(acc_gs)
    taps[...] = jnp.zeros_like(taps)

    def fold(a):
        return a.reshape(TILE // 8, 8, LANES).sum(axis=0)

    def grad_rows(base, size, own=True):
        grads, norms = [], []
        for cb in range(blocks):
            gpre = ga[pl.ds(base, size), lanes(cb)] * dsil[cb, pl.ds(base, size), :]
            nrm = normed[cb, pl.ds(base, size), :]
            if own:
                acc_gs[0, cb] = acc_gs[0, cb] + fold(gpre * nrm)
                acc_gs[1, cb] = acc_gs[1, cb] + fold(gpre)
            grads.append(gpre * gain_ref[0:1, lanes(cb)])
            norms.append(nrm)
        mean = jnp.sum(added(grads), axis=-1, keepdims=True) * (1.0 / channels)
        along = added([a * b for a, b in zip(grads, norms)])
        mean_along = jnp.sum(along, axis=-1, keepdims=True) * (1.0 / channels)
        inv = invs[pl.ds(base, size), :]
        for cb in range(blocks):
            gcr[cb, pl.ds(base, size), :] = inv * (grads[cb] - mean - norms[cb] * mean_along)

    over_tiles(0, n_tiles, grad_rows)
    grad_rows(rows, HALO, own=False)
    beyond = (sp < n_sp - 1).astype(F32)
    for cb in range(blocks):
        gcr[cb, pl.ds(rows, HALO), :] = gcr[cb, pl.ds(rows, HALO), :] * beyond

    def chip_sum(p):
        arrived(("near", p), near_in.at[p])
        arrived(("opp", p), opp_in.at[p])
        total = gsum[p] + near_in[p].astype(F32) + opp_in[p].astype(F32)
        gsum[p] = total
        spread_st[p] = total.astype(BF16)
        for k in ORDER:
            source = spread_st.at[p, chunk_of((mine[p] + k) % SIDE), :]
            send(source, spread_in.at[p, k - 1], around_all[p][k], "spread", "spread")

    phase("chip_sum")
    for p in pieces:
        chip_sum(p)

    def taps_step(i, _):
        base = pl.multiple_of(i * TILE, TILE)
        for cb in range(blocks):
            own = gated[cb, pl.ds(base + HALO, TILE), :]
            for j in range(n_taps):
                shifted = gcr[cb, pl.ds(base + (n_taps - 1 - j), TILE), :]
                taps[cb, j] = taps[cb, j] + fold(own * shifted)
        return 0

    phase("cross_wait")
    arrived("cross", cross_in)
    for p in crossing:
        for owner in range(CHIPS):
            total = cross_own[p - 2, owner, chunk_of(mine[p]), :]
            for k in range(SIDE - 1):
                total = total + cross_in[p - 2, k, owner].astype(F32)
            cross_sum[p - 2, owner] = total
        for k in (2, 1, 3):
            to = (x + k) % CHIPS
            send(cross_sum.at[p - 2, to], cross_x.at[p - 2, k - 1], chip(to), "cross_x", "cross_x")
    phase("taps1")
    lax.fori_loop(0, n_tiles // 2, taps_step, 0)
    phase("taps2")
    lax.fori_loop(n_tiles // 2, n_tiles, taps_step, 0)

    phase("small_fold")
    per_block = SMALL // 8
    row_ids = lax.broadcasted_iota(jnp.int32, (8, LANES), 0)
    for t in range(n_dp * OWN_TILES):
        cb, rb = t // per_block, t % per_block
        tile = jnp.zeros((8, LANES), F32)
        if cb < blocks:
            for r in range(8):
                j = rb * 8 + r
                if j < n_taps:
                    line = taps[cb, j]
                elif j < n_taps + 2:
                    line = acc_gs[j - n_taps, cb]
                else:
                    continue
                line = jnp.sum(line, axis=0, keepdims=True) * scale
                tile = jnp.where(row_ids == r, line, tile)
        sm_all[t // OWN_TILES, t % OWN_TILES] = tile
    for k in range(1, n_dp):
        send(sm_all.at[(dp + k) % n_dp], sm_in.at[k - 1], at_dp[k], "small_0", "small_0")

    def backward_step(i, _):
        base = pl.multiple_of(i * TILE, TILE)
        for cb in range(blocks):
            acc = jnp.zeros((TILE, LANES), F32)
            for j in range(n_taps):
                tap = w_ref[j : j + 1, lanes(cb)]
                acc = acc + tap * gcr[cb, pl.ds(base + (n_taps - 1 - j), TILE), :]
            v = v_ref[pl.ds(base, TILE), lanes(cb)].astype(F32)
            sig = sigmoid(g_ref[pl.ds(base, TILE), lanes(cb)].astype(F32))
            gs = acc * sig
            gv_ref[pl.ds(base, TILE), lanes(cb)] = gs.astype(BF16)
            gg_ref[pl.ds(base, TILE), lanes(cb)] = (gs * v * (1.0 - sig)).astype(BF16)
        return 0

    first = pl.ds(0, SIDE - 1)
    early, late = n_tiles // 2, n_tiles - 1

    phase("backward1")
    lax.fori_loop(0, early, backward_step, 0)

    phase("rs1_wait")
    arrived("spread", spread_in)
    arrived("cross_x", cross_x)
    phase("rs1_sum")

    def first_sum(p, t_ref):
        summed = gsum[p, chunk_of(mine[p]), :]
        for k in range(SIDE - 1):
            summed = summed + spread_in[p, k].astype(F32)
        crossed = cross_sum[p, x]
        for k in range(CHIPS - 1):
            crossed = crossed + cross_x[p, k]
        for c, total in enumerate((summed, crossed)):
            for r in range(part // 8):
                t_ref[2 * r + c] = total[r * 8 : r * 8 + 8, :] * scale

    first_sum(0, t_a)
    first_sum(1, t_b)
    for k in ORDER:
        send(t_a.at[(z + k) % SIDE], rt_a.at[k - 1], at_z[k], "second_a", "tiles")
        send(t_b.at[(y + k) % SIDE], rt_b.at[k - 1], at_y[k], "second_b", "tiles")

    phase("backward2")
    lax.fori_loop(early, late, backward_step, 0)

    phase("small_0")
    arrived("small_0", sm_in)
    total = sm_all[dp]
    for k in range(n_dp - 1):
        total = total + sm_in[k]
    sm_ya[y] = total[:2]
    sm_zb[z] = total[2:]
    for k in ORDER:
        send(sm_ya.at[y], sm_ya.at[y], at_y[k], "small_1a", "small_1")
        send(sm_zb.at[z], sm_zb.at[z], at_z[k], "small_1b", "small_1")

    phase("backward3")
    lax.fori_loop(late, n_tiles, backward_step, 0)

    phase("rs2_wait")
    arrived("second_a", rt_a)
    arrived("second_b", rt_b)
    fin_a[y, z] = t_a[z] + added([rt_a[k] for k in range(SIDE - 1)])
    fin_b[z, y] = t_b[y] + added([rt_b[k] for k in range(SIDE - 1)])
    for k in ORDER:
        send(fin_a.at[y, z], fin_a.at[y, z], at_z[k], ("along_a", k), "tiles")
        send(fin_b.at[z, y], fin_b.at[z, y], at_y[k], ("along_b", k), "tiles")

    def pass_on(a_z, b_y):
        for k in ORDER:
            send(fin_a.at[y, a_z], fin_a.at[y, a_z], at_y[k], "across_a", "across_a")
            send(fin_b.at[z, b_y], fin_b.at[z, b_y], at_z[k], "across_b", "across_b")

    pass_on(z, y)

    phase("small_1")
    arrived("small_1a", sm_ya.at[first])
    arrived("small_1b", sm_zb.at[first])
    sm_za[z] = added([sm_ya[k] for k in range(SIDE)])
    sm_yb[y] = added([sm_zb[k] for k in range(SIDE)])
    for k in ORDER:
        send(sm_za.at[z], sm_za.at[z], at_z[k], "small_2a", "small_2")
        send(sm_yb.at[y], sm_yb.at[y], at_y[k], "small_2b", "small_2")

    phase("ag_pass")
    for k in NEAR_FIRST:
        arrived(("along_a", k), rt_a.at[0])
        arrived(("along_b", k), rt_b.at[0])
        pass_on((z + SIDE - k) % SIDE, (y + SIDE - k) % SIDE)

    phase("small_2")
    arrived("small_2a", sm_za.at[first])
    arrived("small_2b", sm_yb.at[first])
    sm_fin[dp, :2] = added([sm_za[k] for k in range(SIDE)])
    sm_fin[dp, 2:] = added([sm_yb[k] for k in range(SIDE)])
    for k in range(1, n_dp):
        send(sm_fin.at[dp], sm_fin.at[dp], at_dp[k], "small_3", "small_3")

    phase("ag2_wait")
    arrived("across_a", fin_a.at[first])
    arrived("across_b", fin_b.at[first])
    phase("assemble")
    for r in range(SIDE):
        for t in range(SIDE):
            line = slice(r * part + (t // 2) * 8, r * part + (t // 2) * 8 + 8)
            gw_ref[line, lanes(2 * (t % 2))] = fin_a[r, t]
            gw_ref[line, lanes(2 * (t % 2) + 1)] = fin_b[r, t]

    phase("small_3")
    arrived("small_3", sm_fin.at[pl.ds(0, n_dp - 1)])
    for t in range(blocks * per_block):
        cb, rb = t // per_block, t % per_block
        tile = sm_fin[t // OWN_TILES, t % OWN_TILES]
        for first_row, count, out in (
            (0, n_taps, taps_ref), (n_taps, 1, grad_gain), (n_taps + 1, 1, grad_shift)
        ):
            low, high = max(first_row, rb * 8), min(first_row + count, rb * 8 + 8)
            if low < high:
                out[low - first_row : high - first_row, lanes(cb)] = tile[low - rb * 8 : high - rb * 8]
    phase("send_wait")
    left("w", wfull.at[pl.ds(0, 7 * features), :])
    left("cot", cotp)
    left("act", actp)
    left("halo", halo)
    left("next", halo_next)
    left("next_cot", next_rows)
    left("far", far_in)
    left("opp", opp_in)
    left("near", near_in)
    left("spread", spread_in)
    left("cross", cross_in)
    left("cross_x", cross_x)
    left("tiles", fin_a.at[first, pl.ds(0, 4)])
    left("across_a", fin_a.at[first])
    left("across_b", fin_b.at[first])
    for i in range(4):
        left(f"small_{i}", sm_in)
    phase(None)
    assert len(send_ids) == SEND_SEMS and len(receive_ids) == RECEIVE_SEMS


def hand_out(*refs):
    sources, targets, sems = refs[:6], refs[6:12], refs[12]
    copies = [
        pltpu.make_async_copy(a, b, sems.at[i]) for i, (a, b) in enumerate(zip(sources, targets))
    ]
    for copy in copies:
        copy.start()
    for copy in copies:
        copy.wait()


def per_device(count, glu_value, glu_gate, cotangent, conv_weight, norm_gain, norm_shift, out_weight):
    value, gate, cot = glu_value[0], glu_gate[0], cotangent[0]
    rows, channels = value.shape
    n_taps = conv_weight.shape[0]
    features = out_weight.shape[0]
    blocks = channels // LANES
    part = features // SIDE
    n_dp = 2 * CHIPS
    scale = 1.0 / math.sqrt(rows * count)
    hbm = pl.BlockSpec(memory_space=pltpu.HBM)
    anywhere = pl.BlockSpec(memory_space=pl.ANY)
    vmem = pl.BlockSpec(memory_space=pltpu.VMEM)
    shape = jax.ShapeDtypeStruct
    buffer = pltpu.VMEM
    tile = (8, LANES)
    piece = (2, features, LANES)
    outs = pl.pallas_call(
        functools.partial(kernel, scale),
        out_shape=[
            pltpu.VMEM((rows, channels), BF16),
            pltpu.VMEM((rows, channels), BF16),
            pltpu.VMEM((features, channels), F32),
            pltpu.VMEM((n_taps, channels), F32),
            pltpu.VMEM((1, channels), F32),
            pltpu.VMEM((1, channels), F32),
        ],
        in_specs=[hbm] * 7,
        out_specs=[vmem] * 6,
        scratch_shapes=[
            buffer((rows, channels), BF16),
            buffer((rows, channels), BF16),
            buffer((rows + HALO, cot.shape[1]), BF16),
            buffer((n_taps, channels), F32),
            buffer((1, channels), F32),
            buffer((1, channels), F32),
            buffer((features, channels), BF16),
            buffer((2, HALO, channels), BF16),
            buffer((2, HALO, channels), BF16),
            buffer((blocks, rows + 2 * HALO, LANES), F32),
            buffer((blocks, rows + HALO, LANES), F32),
            buffer((rows + HALO, LANES), F32),
            buffer((blocks, rows + HALO, LANES), F32),
            buffer((rows + HALO, channels), F32),
            buffer((blocks, rows + HALO, LANES), F32),
            buffer((rows, channels), BF16),
            buffer((rows, channels), BF16),
            buffer((CHIPS, rows, features), BF16),
            buffer((n_dp * features, channels), BF16),
            buffer(piece, BF16),
            buffer(piece, BF16),
            buffer(piece, BF16),
            buffer(piece, BF16),
            buffer(piece, BF16),
            buffer(piece, BF16),
            buffer(piece, F32),
            buffer((2, features, channels), F32),
            buffer(piece, F32),
            buffer((2, CHIPS, features, LANES), BF16),
            buffer((2, CHIPS, features, LANES), F32),
            buffer((2, SIDE - 1, CHIPS, part, LANES), BF16),
            buffer((2, CHIPS, part, LANES), F32),
            buffer((2, CHIPS - 1, part, LANES), F32),
            buffer(piece, BF16),
            buffer((2, SIDE - 1, part, LANES), BF16),
            buffer((SIDE, *tile), F32),
            buffer((SIDE, *tile), F32),
            buffer((SIDE - 1, *tile), F32),
            buffer((SIDE - 1, *tile), F32),
            buffer((SIDE, SIDE, *tile), F32),
            buffer((SIDE, SIDE, *tile), F32),
            buffer((blocks, n_taps, *tile), F32),
            buffer((2, blocks, *tile), F32),
            buffer((n_dp, OWN_TILES, *tile), F32),
            buffer((n_dp - 1, OWN_TILES, *tile), F32),
            buffer((SIDE, 2, *tile), F32),
            buffer((SIDE, OWN_TILES - 2, *tile), F32),
            buffer((SIDE, 2, *tile), F32),
            buffer((SIDE, OWN_TILES - 2, *tile), F32),
            buffer((n_dp, OWN_TILES, *tile), F32),
            pltpu.SemaphoreType.DMA((SEND_SEMS,)),
            pltpu.SemaphoreType.DMA((RECEIVE_SEMS,)),
            pltpu.SemaphoreType.DMA((7,)),
        ],
        compiler_params=pltpu.CompilerParams(
            collective_id=0, has_side_effects=True, vmem_limit_bytes=62 * 2**20
        ),
        name="backward",
    )(value, gate, cot, conv_weight, norm_gain[None], norm_shift[None], out_weight)
    grad_value, grad_gate, grad_weight, grad_taps, grad_gain, grad_shift = pl.pallas_call(
        hand_out,
        out_shape=[
            shape((rows, channels), BF16),
            shape((rows, channels), BF16),
            shape((features, channels), F32),
            shape((n_taps, channels), F32),
            shape((1, channels), F32),
            shape((1, channels), F32),
        ],
        in_specs=[vmem] * 6,
        out_specs=[anywhere] * 6,
        scratch_shapes=[pltpu.SemaphoreType.DMA((6,))],
        compiler_params=pltpu.CompilerParams(vmem_limit_bytes=16 * 2**20),
        name="hand_out",
    )(*outs)
    return (
        grad_value[None], grad_gate[None], grad_weight,
        grad_taps, grad_gain.reshape(channels), grad_shift.reshape(channels),
    )


def solution(mesh):
    return jax.shard_map(
        functools.partial(per_device, mesh.size),
        mesh=mesh,
        in_specs=(
            P("dp", "sp", None), P("dp", "sp", None), P("dp", "sp", None),
            P(), P(), P(), P("dp", None),
        ),
        out_specs=(P("dp", "sp", None), P("dp", "sp", None), P("dp", None), P(), P(), P()),
        check_vma=False,
    )
```
